256 devices in a mesh: ep: 16 (over y, x), tp: 16 (over z, core).
Axes of the slice: x: 4, y: 4, z: 8, core: 2. Of those that a mesh axis runs over, the one named last changes fastest.
Arguments:
- queries: bfloat16 [8192, 16, 128], P('ep', 'tp'), may hold values from -300 to 300
- keys: bfloat16 [8192, 16, 128], P('ep', 'tp'), may hold values from -4 to 4
- values: bfloat16 [8192, 16, 128], P('ep', 'tp'), may hold values from -6 to 6
- mix_weight: float32 [16], P('tp'), may hold values from 0.3 to 0.8
- sub_gain: float32 [128], replicated, may hold values from 0.1 to 1.9
- tokens: bfloat16 [4096, 2048], P('ep', 'tp'), may hold values from -6 to 6
- routes: int32 [4096, 2], P('ep'), may hold values from 0 to 31, all different within a row; in each aligned block of 256 rows (0 to 255, 256 to 511, ...) at most 24 rows name the same one
- route_weights: float32 [4096, 2], P('ep'), may hold values from 0.1 to 1
- expert_gain: float32 [2048], replicated, may hold values from 0.1 to 1.9
- gate_weight: bfloat16 [32, 2048, 4096], P('ep', None, 'tp'), may hold values from -0.375 to 0.375
- up_weight: bfloat16 [32, 2048, 4096], P('ep', None, 'tp'), may hold values from -0.375 to 0.375
- down_weight: bfloat16 [32, 4096, 2048], P('ep', 'tp'), may hold values from -0.09375 to 0.09375
Outputs:
- attn_out: bfloat16 [8192, 16, 128], P('ep', 'tp')
- moe_out: bfloat16 [4096, 2048], P('ep', 'tp')
The draws below stay inside these ranges and needn't reach their ends.
Inputs may be any that keep to these rules, and one draw needn't show every extreme that they name: `routes`: in each aligned block of 256 rows no expert is named by more than 24 rows, and in every draw some expert is named by exactly 24 rows of some block.
All inputs are finite; a program needn't handle non-finite values.
Results may differ from the reference program's by a relative error of at most 0.018.
Values may be sent and summed in bfloat16 or wider, within the bound.
A program may use at most 128 MiB of HBM per device.

```python
import math
import jax
import jax.numpy as jnp
import numpy as np
from jax import lax

D = 2048
HEADS = 16
HEAD_QK = 64
HEAD_V = 128
FF = 4096
TOPK = 2
ROWS2 = 256
LENGTH = 8192
TOKENS2 = 4096
EXPERTS = 32
CAP = 24
N_EP = 16
N_TP = 16


def paired_fields(key):
    base = jax.random.fold_in(key, 31)
    query_key, field_key = jax.random.split(base, 2)
    shape = (LENGTH, HEADS, 2, HEAD_QK)
    queries = 1.8 * jax.random.truncated_normal(query_key, -4.0, 4.0, shape, jnp.float32)
    keys = jax.random.truncated_normal(field_key, -4.0, 4.0, shape, jnp.float32)
    return (queries.reshape(LENGTH, HEADS, 2 * HEAD_QK), keys.reshape(LENGTH, HEADS, 2 * HEAD_QK))


def draw_queries(key, part):
    return paired_fields(key)[0].astype(jnp.bfloat16)


def draw_keys(key, part):
    return paired_fields(key)[1].astype(jnp.bfloat16)


def block_scale(rng, dims, cuts, smallest, largest):
    def one(axis_at, shards_of):
        draws = jax.random.uniform(jax.random.fold_in(jax.random.fold_in(rng, 6), axis_at), (shards_of,), jnp.float32, smallest / len(cuts), largest / len(cuts))
        return jnp.repeat(jnp.exp(draws), dims[axis_at] // shards_of).reshape((-1,) + (1,) * (len(dims) - axis_at - 1))

    factor_of = one(*cuts[0])
    for cut in cuts[1:]:
        factor_of = factor_of * one(*cut)
    return factor_of


def assign_block(stream_key, own, number, rows, number_of, top, limit, lean):
    order = jax.random.permutation(stream_key, number_of)
    heavy_load, usual = shares(number_of, rows * top, limit, lean, True), shares(number_of, rows * top, limit, lean, False)
    places = jnp.arange(number_of)

    def named(sizes, offset_by):
        used = int((sizes > 0).sum())
        fixed = max(1, used // 4)
        moved = fixed + (places - fixed + offset_by * (used - fixed)) % max(1, number_of - fixed)
        return jnp.zeros((number_of,), jnp.int32).at[order[jnp.where(places < fixed, places, moved)]].set(jnp.asarray(sizes, jnp.int32))

    sizes = jnp.where(number % 4 == 0, named(heavy_load, number // 4), named(usual, number - number // 4 - 1))
    mixed = jax.random.permutation(jax.random.fold_in(own, 3), number_of)
    source_of, sink = mixed[0:number_of // 2 * 2:2], mixed[1:number_of // 2 * 2:2]
    margin = jnp.minimum(sizes[source_of] - 1, limit - sizes[sink]) // 2
    margin = jnp.where((source_of == order[0]) | (sink == order[0]) | (sizes[sink] == 0), 0, jnp.maximum(margin, 0))
    moved = jax.random.randint(jax.random.fold_in(own, 4), (number_of // 2,), 0, 1 << 20) % (margin + 1)
    sizes = sizes.at[source_of].add(-moved).at[sink].add(moved)
    labels = jnp.searchsorted(jnp.cumsum(sizes), jnp.arange(rows * top), side="right").astype(jnp.int32)
    listing = labels.reshape(top, rows).T
    listing = listing[jax.random.permutation(jax.random.fold_in(own, 1), rows)]
    offset_by = jax.random.randint(jax.random.fold_in(own, 2), (rows, 1), 0, top)
    return jnp.take_along_axis(listing, (jnp.arange(top)[None, :] + offset_by) % top, axis=1)


def shares(number_of, total, most, slope, full):
    loads = [(1 << 20) // math.isqrt(grade ** slope) + 1 for grade in range(1, number_of + 1)]
    largest = most if full else min(most, max(-(-total // number_of), total * loads[0] // sum(loads)))
    least = 1 if total - largest >= number_of - 1 else 0
    counts, surplus = [largest] + [least] * (number_of - 1), total - largest - least * (number_of - 1)
    while surplus > 0:
        movable = [i for i in range(1, number_of) if counts[i] < largest] or [i for i in range(1, number_of) if counts[i] < most]
        pool, remaining = sum([loads[i] for i in movable]), surplus
        for i in movable:
            extra = min(most - counts[i], max(1, remaining * loads[i] // pool), surplus)
            counts[i] = counts[i] + extra
            surplus = surplus - extra
    return np.array(counts)


def bell_draw(key, extent, width, bound, pieces=(), kind=jnp.bfloat16):
    entries = jax.random.normal(key, extent, jnp.float32) * width
    if len(pieces) > 0:
        entries = block_scale(key, extent, pieces, -0.22, 0.18) * entries
    return jnp.clip(entries, min=-bound, max=bound).astype(kind)


def setup_inputs(seed: int = 0) -> dict:
    arg_keys = jax.random.split(jax.random.key(seed), 13)
    queries = draw_queries(jax.random.fold_in(arg_keys[12], 71), 0)
    keys = draw_keys(jax.random.fold_in(arg_keys[12], 71), 0)
    values = bell_draw(arg_keys[2], (LENGTH, HEADS, HEAD_V), 1.0, 6.0, ((0, 16), (1, 16)))
    mix_weight = jnp.clip(0.3 + 0.5 * jax.random.uniform(arg_keys[3], (HEADS,), jnp.float32) ** block_scale(arg_keys[3], (HEADS,), ((0, 16),), -0.2, 0.2), 0.3, 0.8)
    sub_gain = jnp.clip(1.0 + 0.18 * jax.random.normal(arg_keys[4], (HEAD_V,), jnp.float32), 0.1, 1.9)
    tokens = bell_draw(arg_keys[5], (TOKENS2, D), 1.0, 6.0, ((0, 16), (1, 16)))
    routes_keys = jax.random.split(jax.random.fold_in(arg_keys[6], 1), TOKENS2 // ROWS2)
    routes_turns = jax.random.permutation(jax.random.fold_in(arg_keys[6], 3), TOKENS2 // ROWS2)
    routes = jax.vmap(lambda own, number: assign_block(jax.random.fold_in(arg_keys[6], 2), own, number, ROWS2, EXPERTS, TOPK, CAP, 1))(routes_keys, routes_turns).reshape((TOKENS2, TOPK))
    route_weights = jnp.clip(0.1 + 0.9 * jax.random.uniform(arg_keys[7], (TOKENS2, TOPK), jnp.float32) ** block_scale(arg_keys[7], (TOKENS2, TOPK), ((0, 16),), -0.2, 0.2), 0.1, 1.0)
    expert_gain = jnp.clip(1.0 + 0.18 * jax.random.normal(arg_keys[8], (D,), jnp.float32), 0.1, 1.9)
    gate_weight = bell_draw(arg_keys[9], (EXPERTS, D, FF), (D // 9) ** -0.5, 0.375, ((0, 16), (2, 16)))
    up_weight = bell_draw(arg_keys[10], (EXPERTS, D, FF), (D // 9) ** -0.5, 0.375, ((0, 16), (2, 16)))
    down_weight = bell_draw(arg_keys[11], (EXPERTS, FF, D), FF ** -0.5, 0.09375, ((0, 16), (1, 16)))
    return {"queries": queries, "keys": keys, "values": values, "mix_weight": mix_weight, "sub_gain": sub_gain, "tokens": tokens, "routes": routes, "route_weights": route_weights, "expert_gain": expert_gain, "gate_weight": gate_weight, "up_weight": up_weight, "down_weight": down_weight}


NEG_FILL = -1e+30
SUB_EPS = 1e-05
NORM_EPS = 1e-06
CLAMP_LIMIT = 7.0
GLU_ALPHA = 1.702
OUT_SCALE = 0.8

def head_attention(bundle, sub_gain):
    head_queries, head_keys, head_values, mix_value = bundle
    block_size = math.gcd(LENGTH, 512)
    key_all = head_keys.reshape(LENGTH, 2, HEAD_QK).astype(jnp.float32)
    key_pos = jnp.arange(LENGTH, dtype=jnp.int32)

    def one_block(block_index):
        offset = block_index * block_size
        query_block = lax.dynamic_slice_in_dim(head_queries, offset, block_size, 0)
        query_block = query_block.reshape(block_size, 2, HEAD_QK).astype(jnp.float32)
        scores = jnp.einsum('qmd,kmd->mqk', query_block, key_all) * HEAD_QK ** (-0.5)
        query_pos = offset + jnp.arange(block_size, dtype=jnp.int32)
        visible = key_pos[None, :] <= query_pos[:, None]
        row_max = lax.optimization_barrier(jnp.max(jnp.where(visible, scores, NEG_FILL), axis=-1))
        weights = jnp.where(visible, jnp.exp(scores - row_max[..., None]), 0.0)
        row_sum = lax.optimization_barrier(jnp.sum(weights, axis=-1))
        rounded = weights.astype(jnp.bfloat16)
        first = jnp.dot(rounded[0], head_values, preferred_element_type=jnp.float32) / row_sum[0][:, None]
        second = jnp.dot(rounded[1], head_values, preferred_element_type=jnp.float32) / row_sum[1][:, None]
        blend = first - mix_value * second
        scaled = blend * lax.rsqrt(lax.optimization_barrier(jnp.mean(blend * blend, axis=-1, keepdims=True)) + SUB_EPS)
        return (scaled * sub_gain * OUT_SCALE).astype(jnp.bfloat16)
    outputs = lax.map(one_block, jnp.arange(LENGTH // block_size, dtype=jnp.int32))
    return outputs.reshape(LENGTH, HEAD_V)

def reference(queries, keys, values, mix_weight, sub_gain, tokens, routes, route_weights, expert_gain, gate_weight, up_weight, down_weight):

    def per_head(bundle):
        return head_attention(bundle, sub_gain)
    heads_all = lax.map(per_head, (jnp.transpose(queries, (1, 0, 2)), jnp.transpose(keys, (1, 0, 2)), jnp.transpose(values, (1, 0, 2)), mix_weight))
    attn_out = jnp.transpose(heads_all, (1, 0, 2))
    floats = tokens.astype(jnp.float32)
    factor = lax.rsqrt(lax.optimization_barrier(jnp.mean(floats * floats, axis=-1)) + NORM_EPS)
    normed = (floats * expert_gain).astype(jnp.bfloat16)
    block_routes = routes.reshape(N_EP, ROWS2 * TOPK)
    onehot = (block_routes[..., None] == jnp.arange(EXPERTS, dtype=jnp.int32)[None, None, :]).astype(jnp.int32)
    slot_rank = lax.optimization_barrier(jnp.sum((jnp.cumsum(onehot, axis=1) - 1) * onehot, axis=2)).astype(jnp.int32)
    target = block_routes * CAP + slot_rank
    token_ids = (jnp.arange(N_EP, dtype=jnp.int32)[:, None] * ROWS2 + jnp.arange(ROWS2 * TOPK, dtype=jnp.int32)[None, :] // TOPK).astype(jnp.int32)
    block_ids = jnp.broadcast_to(jnp.arange(N_EP, dtype=jnp.int32)[:, None], target.shape)
    slot_owner = jnp.full((N_EP, EXPERTS * CAP), TOKENS2, jnp.int32).at[block_ids, target].set(token_ids)
    slot_owner = jnp.transpose(slot_owner.reshape(N_EP, EXPERTS, CAP), (1, 0, 2)).reshape(EXPERTS, N_EP * CAP)
    padded_rows = jnp.concatenate([normed, jnp.zeros((1, D), jnp.bfloat16)], axis=0)
    padded_factor = jnp.concatenate([factor, jnp.zeros((1,), jnp.float32)], axis=0)

    def run_expert(bundle):
        slot_list, expert_gate, expert_up, expert_down = bundle
        rows_in = padded_rows[slot_list]
        scale = padded_factor[slot_list][:, None]
        gate_pre = jnp.minimum(jnp.dot(rows_in, expert_gate, preferred_element_type=jnp.float32) * scale, CLAMP_LIMIT)
        up_pre = jnp.clip(jnp.dot(rows_in, expert_up, preferred_element_type=jnp.float32) * scale, -CLAMP_LIMIT, CLAMP_LIMIT)
        hidden = ((up_pre + 1.0) * gate_pre * jax.nn.sigmoid(GLU_ALPHA * gate_pre)).astype(jnp.bfloat16)
        hidden_parts = hidden.reshape(N_EP * CAP, N_TP, FF // N_TP)
        down_parts = expert_down.reshape(N_TP, FF // N_TP, D)

        def add_part(part_index, running):
            piece = jnp.dot(hidden_parts[:, part_index], down_parts[part_index], preferred_element_type=jnp.float32).astype(jnp.bfloat16)
            piece = lax.optimization_barrier(piece)
            return running + piece.astype(jnp.float32)
        summed = lax.fori_loop(0, N_TP, add_part, jnp.zeros((N_EP * CAP, D), jnp.float32))
        return summed.astype(jnp.bfloat16)
    expert_rows = lax.map(run_expert, (slot_owner, gate_weight, up_weight, down_weight)).reshape(EXPERTS, N_EP, CAP, D)
    row_block = (jnp.arange(TOKENS2, dtype=jnp.int32) // ROWS2)[:, None]
    picked = expert_rows[routes, jnp.broadcast_to(row_block, routes.shape), slot_rank.reshape(TOKENS2, TOPK)]
    moe_out = lax.optimization_barrier(jnp.sum(picked.astype(jnp.float32) * route_weights[..., None], axis=1)).astype(jnp.bfloat16)
    return (attn_out, moe_out)
```

```python
import functools
import math

import jax
import jax.numpy as jnp
from jax import lax
from jax.experimental import pallas as pl
from jax.experimental.pallas import tpu as pltpu
from jax.sharding import PartitionSpec as P

MESH = pl.DeviceIdType.MESH
NEG_FILL = -1e30
SUB_EPS = 1e-05
NORM_EPS = 1e-06
CLAMP_LIMIT = 7.0
GLU_ALPHA = 1.702
OUT_SCALE = 0.8
AG_CUTS = 4
F32 = jnp.float32
BF16 = jnp.bfloat16


def nt_dot(a, b):
    return lax.dot_general(a, b, (((1,), (1,)), ((), ())), preferred_element_type=F32)


def tn_dot(a, b):
    return lax.dot_general(a, b, (((0,), (0,)), ((), ())), preferred_element_type=F32)


def nn_dot(a, b):
    return jnp.dot(a, b, preferred_element_type=F32)


def kernel(
    cfg,
    q_ref,
    k_ref,
    v_ref,
    mix_ref,
    sub_gain_ref,
    tokens_ref,
    routes_ref,
    pick_weight_ref,
    gain_ref,
    gate_hbm,
    up_hbm,
    down_hbm,
    attn_ref,
    moe_ref,
    qz,
    kbuf,
    vbuf,
    acc,
    row_max,
    picks,
    outgoing,
    gathered,
    gate_w,
    up_w,
    down_w,
    pre,
    squares,
    hidden,
    ybuf,
    prec,
    rsend,
    rrecv,
    back_send,
    back,
    w_sem,
    k_send,
    k_recv,
    v_send,
    v_recv,
    d_send,
    d_recv,
    g_send,
    g_recv,
    p_send,
    p_recv,
    y_send,
    y_recv,
    r_send,
    r_recv,
    b_send,
    b_recv,
):
    n_ep, n_tp, cap, rows = cfg["n_ep"], cfg["n_tp"], cfg["cap"], cfg["rows"]
    n_z = n_tp // 2
    block = 2 * cap
    slots = n_ep * block
    half = slots // 2
    sources_half = n_ep // 2
    per_expert = half // 2
    ep = lax.axis_index("ep")
    tp = lax.axis_index("tp")
    z, c = lax.div(tp, 2), lax.rem(tp, 2)
    partner = tp + 1 - 2 * c

    def ring(at, shift):
        return lax.rem(at + shift + 2 * n_z, n_z)

    def remote(src, dst, send_sem, recv_sem, to_ep, to_tp):
        return pltpu.make_async_remote_copy(
            src_ref=src,
            dst_ref=dst,
            send_sem=send_sem,
            recv_sem=recv_sem,
            device_id=(to_ep, to_tp),
            device_id_type=MESH,
        )

    barrier = pltpu.get_barrier_semaphore()
    for off in range(1, n_ep):
        pl.semaphore_signal(
            barrier, inc=1, device_id=(lax.rem(ep + off, n_ep), tp), device_id_type=MESH
        )
    for to in (2 * ring(z, 1) + c, 2 * ring(z, -1) + c, partner):
        pl.semaphore_signal(barrier, inc=1, device_id=(ep, to), device_id_type=MESH)

    weight_copies = [
        pltpu.make_async_copy(gate_hbm, gate_w, w_sem.at[0]),
        pltpu.make_async_copy(up_hbm, up_w, w_sem.at[1]),
        pltpu.make_async_copy(down_hbm, down_w, w_sem.at[2]),
    ]
    for copy in weight_copies:
        copy.start()

    pairs = 2 * rows
    experts = 2 * n_ep
    routes = routes_ref[...]
    member = (
        lax.broadcasted_iota(jnp.int32, (experts, pairs), 0)
        == jnp.broadcast_to(routes, (experts, pairs))
    ).astype(F32)

    def order(dim):
        at = lax.broadcasted_iota(jnp.int32, (pairs, pairs), dim)
        return jnp.where(at < rows, 2 * at, 2 * (at - rows) + 1)

    earlier = (order(0) < order(1)).astype(F32).astype(BF16)
    rank = nn_dot(member.astype(BF16), earlier)
    first_slot = lax.broadcasted_iota(jnp.int32, (experts, pairs), 0).astype(F32) * float(cap)
    target = jnp.sum(member * (rank + first_slot), axis=0, keepdims=True)
    slot_at = lax.broadcasted_iota(jnp.int32, (slots, rows), 0).astype(F32)
    pick_0 = (slot_at == jnp.broadcast_to(target[:, :rows], (slots, rows))).astype(F32)
    pick_1 = (slot_at == jnp.broadcast_to(target[:, rows:], (slots, rows))).astype(F32)
    picks[0] = pick_0.astype(BF16)
    picks[1] = pick_1.astype(BF16)
    out_rows = nn_dot((pick_0 + pick_1).astype(BF16), tokens_ref[...]).astype(BF16)
    outgoing[...] = out_rows
    mine = pl.ds(pl.multiple_of(ep * block, block), block)
    gathered[tp, mine, :] = outgoing[mine, :]

    q_all = q_ref[...]
    q_rows = q_all.shape[0]
    lane = lax.broadcasted_iota(jnp.int32, q_all.shape, 1)
    zero = jnp.zeros_like(q_all)
    qz[:q_rows] = jnp.where(lane < q_all.shape[1] // 2, q_all, zero)
    qz[q_rows:] = jnp.where(lane >= q_all.shape[1] // 2, q_all, zero)

    pl.semaphore_wait(barrier, n_ep - 1 + 3)

    def dispatch_copy(off):
        to = lax.rem(ep + off, n_ep)
        return remote(
            outgoing.at[pl.ds(pl.multiple_of(to * block, block), block)],
            gathered.at[tp, mine],
            d_send.at[off],
            d_recv.at[off],
            to,
            tp,
        )

    for off in range(1, n_ep):
        dispatch_copy(off).start()

    def key_copy(off):
        return remote(k_ref, kbuf.at[off], k_send.at[off], k_recv.at[off], ep + off, tp)

    def value_copy(off):
        return remote(v_ref, vbuf.at[off], v_send.at[off], v_recv.at[off], ep + off, tp)

    @pl.loop(1, n_ep)
    def _(off):
        @pl.when(ep + off < n_ep)
        def _():
            key_copy(off).start()
            value_copy(off).start()

    exponent = (q_ref.shape[1] // 2) ** (-0.5) * math.log2(math.e)
    width = v_ref.shape[1]
    tile = min(256, q_rows)

    def attend(keys, values, first):
        both = jnp.concatenate([values, jnp.ones_like(values)], axis=1)
        for r in range(0, 2 * q_rows, tile):
            at = pl.ds(r, tile)
            scores = nt_dot(qz[at, :], keys)
            if first:
                seen = lax.broadcasted_iota(jnp.int32, scores.shape, 1) <= (
                    lax.broadcasted_iota(jnp.int32, scores.shape, 0) + r % q_rows
                )
                scores = jnp.where(seen, scores, NEG_FILL)
                top = jnp.broadcast_to(jnp.max(scores, axis=1, keepdims=True), (tile, 128))
            else:
                old = row_max[at, :]
                top = jnp.maximum(old, jnp.max(scores, axis=1, keepdims=True))
            weights = jnp.exp2((scores - top[:, :1]) * exponent).astype(BF16)
            part = nn_dot(weights, both)
            if first:
                acc[at, :] = part
            else:
                shrink = jnp.exp2((old - top) * exponent)
                acc[at, :] = acc[at, :] * jnp.concatenate([shrink, shrink], axis=1) + part
            row_max[at, :] = top

    def attend_step(off):
        @pl.when(ep >= off)
        def _():
            remote(k_ref, kbuf.at[off], k_send.at[off], k_recv.at[off], ep, partner).wait_recv()
            remote(v_ref, vbuf.at[off], v_send.at[off], v_recv.at[off], ep, partner).wait_recv()
            attend(kbuf[off], vbuf[off], False)

    attend(k_ref[...], v_ref[...], True)

    cut = half // AG_CUTS

    def gather_copy(h, hop, sub):
        source = ring(z, -hop) if h == 0 else ring(z, hop)
        to = ring(z, 1) if h == 0 else ring(z, -1)
        piece = gathered.at[2 * source + c, pl.ds(h * half + sub * cut, cut)]
        at = (h * n_z + hop) * AG_CUTS + sub
        return remote(piece, piece, g_send.at[at], g_recv.at[at], ep, 2 * to + c)

    def gather_wait(h, hop, sub):
        source = ring(z, -hop) if h == 0 else ring(z, hop)
        piece = gathered.at[2 * source + c, pl.ds(h * half + sub * cut, cut)]
        at = (h * n_z + hop - 1) * AG_CUTS + sub
        remote(piece, piece, g_send.at[at], g_recv.at[at], ep, partner).wait_recv()

    def partner_copy(h, hop, mine_or_theirs):
        source = ring(z, -hop) if h == 0 else ring(z, hop)
        piece = gathered.at[2 * source + mine_or_theirs, pl.ds(h * half, half)]
        at = h * n_z + hop
        return remote(piece, piece, p_send.at[at], p_recv.at[at], ep, partner)

    for h in range(2):
        for s in range(h * sources_half, (h + 1) * sources_half):

            @pl.when(ep != s)
            def _(s=s):
                off = lax.rem(ep - s + n_ep, n_ep)
                piece = gathered.at[tp, pl.ds(s * block, block)]
                remote(piece, piece, d_send.at[off], d_recv.at[off], s, tp).wait_recv()

        for sub in range(AG_CUTS):
            gather_copy(h, 0, sub).start()
        partner_copy(h, 0, c).start()

    for copy in weight_copies:
        copy.wait()

    def by_expert(value):
        w = value.shape[1]
        cut_up = value.reshape(sources_half, 2, cap, w)
        return [cut_up[:, e].reshape(per_expert, w) for e in range(2)]

    def expert_in(hop, first):
        for h in range(2):
            source = ring(z, -hop) if h == 0 else ring(z, hop)
            partner_copy(h, hop, 1 - c).wait_recv()
            at = pl.ds(h * half, half)
            x = jnp.concatenate(
                [gathered[2 * source, at, :], gathered[2 * source + 1, at, :]], axis=1
            ).astype(F32)
            square = jnp.broadcast_to(jnp.sum(x * x, axis=1, keepdims=True), (half, 128))
            squares[h] = square if first else squares[h] + square
            depth = x.shape[1]
            deep = pl.ds(pl.multiple_of(source * depth, depth), depth)
            for e, rows_e in enumerate(by_expert(x * gain_ref[source])):
                rows_e = rows_e.astype(BF16)
                for n, w in enumerate((gate_w, up_w)):
                    product = nn_dot(rows_e, w[e, deep, :])
                    pre[h, e, n] = product if first else pre[h, e, n] + product

    for hop in range(1, n_z):
        for sub in range(AG_CUTS):
            for h in range(2):
                gather_wait(h, hop, sub)
                if hop < n_z - 1:
                    gather_copy(h, hop, sub).start()
        for h in range(2):
            partner_copy(h, hop, c).start()
        expert_in(hop - 1, hop == 1)
    expert_in(n_z - 1, False)

    for h in range(2):
        factor = lax.rsqrt(squares[h] / float(cfg["width"]) + NORM_EPS)
        for e, f in enumerate(by_expert(factor)):
            f = jnp.concatenate([f, f], axis=1)
            gate = jnp.minimum(pre[h, e, 0] * f, CLAMP_LIMIT)
            up = jnp.clip(pre[h, e, 1] * f, -CLAMP_LIMIT, CLAMP_LIMIT)
            hidden[h, e] = ((up + 1.0) * gate * jax.nn.sigmoid(GLU_ALPHA * gate)).astype(BF16)

    def down(hop):
        for h in range(2):
            goal = ring(z, -1 - hop) if h == 0 else ring(z, 1 + hop)
            wide = pl.ds(pl.multiple_of(goal * 256, 256), 256)
            for e in range(2):
                y = nn_dot(hidden[h, e], down_w[e, :, wide]).astype(BF16)
                ybuf[0, h, hop, e] = y[:, :128]
                ybuf[1, h, hop, e] = y[:, 128:]

    def y_copy(h, hop):
        at = h * n_z + hop
        return remote(
            ybuf.at[1 - c, h, hop], prec.at[h, hop], y_send.at[at], y_recv.at[at], ep, partner
        )

    def sum_copy(h, hop, e):
        to = ring(z, 1) if h == 0 else ring(z, -1)
        at = (h * n_z + hop) * 2 + e
        return remote(
            rsend.at[h, hop, e], rrecv.at[h, hop, e], r_send.at[at], r_recv.at[at], ep, 2 * to + c
        )

    def own_sum(h, hop, e):
        return ybuf[c, h, hop, e].astype(F32) + prec[h, hop, e].astype(F32)

    for hop in range(n_z):
        down(hop)
        for h in range(2):
            y_copy(h, hop).start()
    for h in range(2):
        y_copy(h, 0).wait_recv()
        for e in range(2):
            rsend[h, 0, e] = own_sum(h, 0, e).astype(BF16)
            sum_copy(h, 0, e).start()

    @pl.loop(1, n_ep)
    def _(off):
        attend_step(off)

    for hop in range(1, n_z - 1):
        for h in range(2):
            y_copy(h, hop).wait_recv()
        for e in range(2):
            for h in range(2):
                sum_copy(h, hop - 1, e).wait_recv()
                total = own_sum(h, hop, e) + rrecv[h, hop - 1, e].astype(F32)
                rsend[h, hop, e] = total.astype(BF16)
                sum_copy(h, hop, e).start()

    def back_copy(s):
        off = lax.rem(s - ep + n_ep, n_ep)
        return remote(
            back_send.at[pl.ds(s * block, block)],
            back.at[mine],
            b_send.at[off],
            b_recv.at[off],
            s,
            tp,
        )

    last = n_z - 1
    for h in range(2):
        y_copy(h, last).wait_recv()
        totals = []
        for e in range(2):
            sum_copy(h, last - 1, e).wait_recv()
            total = own_sum(h, last, e) + rrecv[h, last - 1, e].astype(F32)
            totals.append(total.reshape(sources_half, 1, cap, 128))
        back_send[h * half : (h + 1) * half] = (
            jnp.concatenate(totals, axis=1).reshape(half, 128).astype(BF16)
        )
        for s in range(h * sources_half, (h + 1) * sources_half):

            @pl.when(ep != s)
            def _(s=s):
                back_copy(s).start()

    back[mine, :] = back_send[mine, :]

    mix = mix_ref[0, 0]
    for r in range(0, q_rows, tile):
        one, two = pl.ds(r, tile), pl.ds(q_rows + r, tile)
        blend = acc[one, :width] / acc[one, width:] - mix * (acc[two, :width] / acc[two, width:])
        mean = jnp.mean(blend * blend, axis=1, keepdims=True)
        scaled = blend * lax.rsqrt(mean + SUB_EPS)
        attn_ref[one, :] = (scaled * sub_gain_ref[...] * OUT_SCALE).astype(BF16)

    for off in range(1, n_ep):
        piece = back.at[mine]
        remote(piece, piece, b_send.at[off], b_recv.at[off], ep, partner).wait_recv()
    result = back[...]
    weight = pick_weight_ref[...]
    moe_ref[...] = (
        tn_dot(picks[0], result) * weight[:, :1] + tn_dot(picks[1], result) * weight[:, 1:]
    ).astype(BF16)

    for off in range(1, n_ep):
        dispatch_copy(off).wait_send()
        back_copy(lax.rem(ep + off, n_ep)).wait_send()

    @pl.loop(1, n_ep)
    def _(off):
        @pl.when(ep + off < n_ep)
        def _():
            key_copy(off).wait_send()
            value_copy(off).wait_send()

    for h in range(2):
        for hop in range(n_z):
            partner_copy(h, hop, c).wait_send()
            y_copy(h, hop).wait_send()
            if hop < n_z - 1:
                for sub in range(AG_CUTS):
                    gather_copy(h, hop, sub).wait_send()
                for e in range(2):
                    sum_copy(h, hop, e).wait_send()


def shards(
    queries,
    keys,
    values,
    mix_weight,
    sub_gain,
    tokens,
    routes,
    route_weights,
    expert_gain,
    gate_weight,
    up_weight,
    down_weight,
):
    n_ep, n_tp = lax.axis_size("ep"), lax.axis_size("tp")
    n_z = n_tp // 2
    rows, pick_count = routes.shape
    experts = n_ep * gate_weight.shape[0]
    cap = 3 * rows * pick_count // (2 * experts)
    slots = experts * cap
    half = slots // 2
    q_rows, _, qk_width = queries.shape
    v_width = values.shape[2]
    width = expert_gain.shape[0]
    ff = gate_weight.shape[2]
    cfg = dict(n_ep=n_ep, n_tp=n_tp, cap=cap, rows=rows, width=width)
    dma = pltpu.SemaphoreType.DMA
    vmem = pl.BlockSpec(memory_space=pltpu.VMEM)
    anywhere = pl.BlockSpec(memory_space=pl.ANY)
    attn_out, moe_out = pl.pallas_call(
        functools.partial(kernel, cfg),
        name="layer",
        out_shape=(
            jax.ShapeDtypeStruct((q_rows, v_width), BF16),
            jax.ShapeDtypeStruct((rows, tokens.shape[1]), BF16),
        ),
        in_specs=[vmem] * 3
        + [pl.BlockSpec(memory_space=pltpu.SMEM)]
        + [vmem] * 5
        + [anywhere] * 3,
        out_specs=(vmem, vmem),
        scratch_shapes=[
            pltpu.VMEM((2 * q_rows, qk_width), BF16),
            pltpu.VMEM((n_ep, q_rows, qk_width), BF16),
            pltpu.VMEM((n_ep, q_rows, v_width), BF16),
            pltpu.VMEM((2 * q_rows, 2 * v_width), F32),
            pltpu.VMEM((2 * q_rows, 128), F32),
            pltpu.VMEM((2, slots, rows), BF16),
            pltpu.VMEM((slots, tokens.shape[1]), BF16),
            pltpu.VMEM((n_tp, slots, tokens.shape[1]), BF16),
            pltpu.VMEM(gate_weight.shape, BF16),
            pltpu.VMEM(up_weight.shape, BF16),
            pltpu.VMEM(down_weight.shape, BF16),
            pltpu.VMEM((2, 2, 2, half // 2, ff), F32),
            pltpu.VMEM((2, half, 128), F32),
            pltpu.VMEM((2, 2, half // 2, ff), BF16),
            pltpu.VMEM((2, 2, n_z, 2, half // 2, 128), BF16),
            pltpu.VMEM((2, n_z, 2, half // 2, 128), BF16),
            pltpu.VMEM((2, n_z - 1, 2, half // 2, 128), BF16),
            pltpu.VMEM((2, n_z - 1, 2, half // 2, 128), BF16),
            pltpu.VMEM((slots, 128), BF16),
            pltpu.VMEM((slots, 128), BF16),
            dma((3,)),
            dma((n_ep,)),
            dma((n_ep,)),
            dma((n_ep,)),
            dma((n_ep,)),
            dma((n_ep,)),
            dma((n_ep,)),
            dma((2 * n_z * AG_CUTS,)),
            dma((2 * n_z * AG_CUTS,)),
            dma((2 * n_z,)),
            dma((2 * n_z,)),
            dma((2 * n_z,)),
            dma((2 * n_z,)),
            dma((2 * n_z * 2,)),
            dma((2 * n_z * 2,)),
            dma((n_ep,)),
            dma((n_ep,)),
        ],
        compiler_params=pltpu.CompilerParams(
            collective_id=0, has_side_effects=True, vmem_limit_bytes=60 * 1024 * 1024
        ),
    )(
        queries.reshape(q_rows, qk_width),
        keys.reshape(q_rows, qk_width),
        values.reshape(q_rows, v_width),
        mix_weight.reshape(1, 1),
        sub_gain.reshape(1, v_width),
        tokens,
        routes.T.reshape(1, 2 * rows),
        route_weights,
        expert_gain.reshape(n_z, 1, width // n_z),
        gate_weight,
        up_weight,
        down_weight,
    )
    return attn_out.reshape(q_rows, 1, v_width), moe_out


def solution(mesh):
    return jax.shard_map(
        shards,
        mesh=mesh,
        in_specs=(
            P("ep", "tp", None),
            P("ep", "tp", None),
            P("ep", "tp", None),
            P("tp"),
            P(),
            P("ep", "tp"),
            P("ep", None),
            P("ep", None),
            P(),
            P("ep", None, "tp"),
            P("ep", None, "tp"),
            P("ep", "tp", None),
        ),
        out_specs=(P("ep", "tp", None), P("ep", "tp")),
        check_vma=False,
    )
```

```python
import functools
import math

import jax
import jax.numpy as jnp
from jax import lax
from jax.experimental import pallas as pl
from jax.experimental.pallas import tpu as pltpu
from jax.sharding import PartitionSpec as P

MESH = pl.DeviceIdType.MESH
NEG_FILL = -1e30
SUB_EPS = 1e-05
NORM_EPS = 1e-06
CLAMP_LIMIT = 7.0
GLU_ALPHA = 1.702
OUT_SCALE = 0.8
F32 = jnp.float32
BF16 = jnp.bfloat16


def nt_dot(a, b):
    return lax.dot_general(a, b, (((1,), (1,)), ((), ())), preferred_element_type=F32)


def tn_dot(a, b):
    return lax.dot_general(a, b, (((0,), (0,)), ((), ())), preferred_element_type=F32)


def nn_dot(a, b):
    return jnp.dot(a, b, preferred_element_type=F32)


STAGES = (
    ((), (((0, 0), "x+"), ((0, 0), "x-"), ((0, 0), "y+"), ((0, 0), "y-"))),
    (
        ((0, -1), (0, 1), (-1, 0), (1, 0)),
        (
            ((0, -1), "x+"),
            ((0, -1), "y+"),
            ((0, -1), "y-"),
            ((0, 1), "y+"),
            ((0, 1), "y-"),
            ((-1, 0), "y+"),
        ),
    ),
    (
        ((0, 2), (-1, -1), (1, -1), (-1, 1), (1, 1), (2, 0)),
        (((0, 2), "y+"), ((0, 2), "y-"), ((-1, -1), "y+"), ((1, 1), "y-")),
    ),
    (((-1, 2), (1, 2), (2, -1), (2, 1)), (((1, 2), "y-"),)),
    (((2, 2),), ()),
)
STEP = {"x+": (0, 1), "x-": (0, -1), "y+": (1, 0), "y-": (-1, 0)}
MIRROR = {"x+": "y-", "x-": "y+", "y+": "x-", "y-": "x+"}
SIDE = 4


def kernel(
    cfg,
    q_hbm,
    k_hbm,
    v_hbm,
    mix_hbm,
    sub_gain_hbm,
    tokens_hbm,
    routes_hbm,
    pick_weight_hbm,
    gain_hbm,
    gate_hbm,
    up_hbm,
    down_hbm,
    attn_hbm,
    moe_hbm,
    q_ref,
    mix_ref,
    sub_gain_ref,
    tokens_ref,
    routes_ref,
    pick_weight_ref,
    gain_ref,
    gate_w,
    up_w,
    down_w,
    attn_ref,
    moe_ref,
    qz,
    kbuf,
    vbuf,
    acc,
    row_max,
    picks,
    outgoing,
    gathered,
    pre,
    squares,
    hidden,
    ybuf,
    prec,
    rsend,
    rrecv,
    back_send,
    back,
    in_sem,
    out_sem,
    kv_send,
    kv_recv,
    d_sem,
    g_send,
    g_recv,
    p_send,
    p_recv,
    y_send,
    y_recv,
    r_send,
    r_recv,
    b_sem,
):
    n_ep, n_tp, cap, rows = cfg["n_ep"], cfg["n_tp"], cfg["cap"], cfg["rows"]
    n_z = n_tp // 2
    far = n_z // 2
    block = 2 * cap
    slots = n_ep * block
    half = slots // 2
    sources_half = n_ep // 2
    part = half // 2
    ep = lax.axis_index("ep")
    tp = lax.axis_index("tp")
    z, c = lax.div(tp, 2), lax.rem(tp, 2)
    py, px = lax.div(ep, SIDE), lax.rem(ep, SIDE)
    partner = tp + 1 - 2 * c

    def ring(at, shift):
        return lax.rem(at + shift + 2 * n_z, n_z)

    def remote(src, dst, send_sem, recv_sem, to_ep, to_tp):
        return pltpu.make_async_remote_copy(
            src_ref=src,
            dst_ref=dst,
            send_sem=send_sem,
            recv_sem=recv_sem,
            device_id=(to_ep, to_tp),
            device_id_type=MESH,
        )

    barrier = pltpu.get_barrier_semaphore()
    for off in range(1, n_ep):
        pl.semaphore_signal(
            barrier, inc=1, device_id=(lax.rem(ep + off, n_ep), tp), device_id_type=MESH
        )
    for to in (2 * ring(z, 1) + c, 2 * ring(z, -1) + c, partner):
        pl.semaphore_signal(barrier, inc=1, device_id=(ep, to), device_id_type=MESH)

    loads = [
        pltpu.make_async_copy(src, dst, in_sem.at[i])
        for i, (src, dst) in enumerate(
            (
                (routes_hbm, routes_ref),
                (tokens_hbm, tokens_ref),
                (q_hbm, q_ref),
                (k_hbm, kbuf.at[0]),
                (v_hbm, vbuf.at[0]),
                (gain_hbm, gain_ref),
                (gate_hbm, gate_w),
                (up_hbm, up_w),
                (down_hbm, down_w),
                (mix_hbm, mix_ref),
                (sub_gain_hbm, sub_gain_ref),
                (pick_weight_hbm, pick_weight_ref),
            )
        )
    ]
    for copy in loads:
        copy.start()

    for copy in loads[:2]:
        copy.wait()
    pairs = 2 * rows
    experts = 2 * n_ep
    routes = jnp.concatenate([routes_ref[0:1, :], routes_ref[1:2, :]], axis=1)
    member = (
        lax.broadcasted_iota(jnp.int32, (experts, pairs), 0)
        == jnp.broadcast_to(routes, (experts, pairs))
    ).astype(F32)

    def order(dim):
        at = lax.broadcasted_iota(jnp.int32, (pairs, pairs), dim)
        return jnp.where(at < rows, 2 * at, 2 * (at - rows) + 1)

    earlier = (order(0) < order(1)).astype(F32).astype(BF16)
    rank = nn_dot(member.astype(BF16), earlier)
    first_slot = lax.broadcasted_iota(jnp.int32, (experts, pairs), 0).astype(F32) * float(cap)
    target = jnp.sum(member * (rank + first_slot), axis=0, keepdims=True)
    slot_at = lax.broadcasted_iota(jnp.int32, (slots, rows), 0).astype(F32)
    pick_0 = (slot_at == jnp.broadcast_to(target[:, :rows], (slots, rows))).astype(F32)
    pick_1 = (slot_at == jnp.broadcast_to(target[:, rows:], (slots, rows))).astype(F32)
    picks[0] = pick_0.astype(BF16)
    picks[1] = pick_1.astype(BF16)
    out_rows = nn_dot((pick_0 + pick_1).astype(BF16), tokens_ref[...]).astype(BF16)
    outgoing[...] = out_rows
    mine = pl.ds(pl.multiple_of(ep * block, block), block)
    gathered[tp, mine, :] = outgoing[mine, :]

    loads[2].wait()
    q_all = q_ref[...]
    q_rows = q_all.shape[0]
    lane = lax.broadcasted_iota(jnp.int32, q_all.shape, 1)
    zero = jnp.zeros_like(q_all)
    qz[:q_rows] = jnp.where(lane < q_all.shape[1] // 2, q_all, zero)
    qz[q_rows:] = jnp.where(lane >= q_all.shape[1] // 2, q_all, zero)

    pl.semaphore_wait(barrier, n_ep - 1 + 3)

    for off in range(1, n_ep):
        to = lax.rem(ep + off, n_ep)
        remote(
            outgoing.at[pl.ds(pl.multiple_of(to * block, block), block)],
            gathered.at[tp, mine],
            d_sem.at[0],
            d_sem.at[1],
            to,
            tp,
        ).start()
    others = (n_ep - 1) * block

    exponent = (q_ref.shape[1] // 2) ** (-0.5) * math.log2(math.e)
    width = vbuf.shape[2]
    tile = min(256, q_rows)

    def scores_at(r, keys, first):
        scores = nt_dot(qz[pl.ds(r, tile), :], keys)
        if first:
            seen = lax.broadcasted_iota(jnp.int32, scores.shape, 1) <= (
                lax.broadcasted_iota(jnp.int32, scores.shape, 0) + r % q_rows
            )
            scores = jnp.where(seen, scores, NEG_FILL)
        return scores

    def attend(held, maps=(0, 1), first=False):
        keys = jnp.concatenate([kbuf[s] for s in held], axis=0)
        values = jnp.concatenate([vbuf[s] for s in held], axis=0)
        both = jnp.concatenate([values, jnp.ones_like(values)], axis=1)
        at = [m * q_rows + r for m in maps for r in range(0, q_rows, tile)]
        scores = [scores_at(r, keys, first) for r in at]
        tops = [jnp.max(s, axis=1, keepdims=True) for s in scores]
        if first:
            tops = [jnp.broadcast_to(t, (tile, 128)) for t in tops]
        else:
            olds = [row_max[pl.ds(r, tile), :] for r in at]
            tops = [jnp.maximum(o, t) for o, t in zip(olds, tops)]
        weights = [
            jnp.exp2((s - t[:, :1]) * exponent).astype(BF16) for s, t in zip(scores, tops)
        ]
        for i, r in enumerate(at):
            where = pl.ds(r, tile)
            added = nn_dot(weights[i], both)
            if first:
                acc[where, :] = added
            else:
                shrink = jnp.exp2((olds[i] - tops[i]) * exponent)
                acc[where, :] = acc[where, :] * jnp.concatenate([shrink, shrink], axis=1) + added
            row_max[where, :] = tops[i]

    def held_at(a, b):
        return (a % SIDE) * SIDE + b % SIDE

    def spread(stage):
        waits, sends = STAGES[stage]
        for n, buf in enumerate((kbuf, vbuf)):
            for a, b in waits:
                at = held_at(a, b) if n == 0 else held_at(-b, -a)
                remote(
                    buf.at[at], buf.at[at], kv_send.at[n], kv_recv.at[n, at], ep, partner
                ).wait_recv()
        for (a, b), way in sends:
            for n, buf in enumerate((kbuf, vbuf)):
                if n == 1:
                    a, b, way = -b, -a, MIRROR[way]
                dy, dx = STEP[way]
                to = lax.rem(py + dy + SIDE, SIDE) * SIDE + lax.rem(px + dx + SIDE, SIDE)
                at = held_at(a - dy, b - dx)
                remote(
                    buf.at[held_at(a, b)], buf.at[at], kv_send.at[n], kv_recv.at[n, at], to, tp
                ).start()

    for copy in loads[3:5]:
        copy.wait()
    attend((0,), first=True)
    spread(0)

    arrived = gathered.at[tp, pl.ds(0, others)]
    remote(arrived, arrived, d_sem.at[0], d_sem.at[1], ep, partner).wait_recv()

    cut = half // 2

    def source_of(way, hop):
        return ring(z, -hop) if way == 0 else ring(z, hop)

    def gather_copy(way, hop, sub):
        to = ring(z, 1) if way == 0 else ring(z, -1)
        piece = gathered.at[2 * source_of(way, hop) + c, pl.ds(sub * cut, cut)]
        at = (way * far + hop) * 4 + sub
        return remote(piece, piece, g_send.at[0], g_recv.at[at], ep, 2 * to + c)

    def gather_wait(way, hop, sub):
        piece = gathered.at[2 * source_of(way, hop) + c, pl.ds(sub * cut, cut)]
        at = (way * far + hop - 1) * 4 + sub
        remote(piece, piece, g_send.at[0], g_recv.at[at], ep, partner).wait_recv()

    def subs_of(way, hop):
        return range(4) if hop < far - 1 else range(2 * way, 2 * way + 2)

    def shard(way, hop):
        return 0 if hop == 0 else (2 * hop - 1 + way if hop < far else n_z - 1)

    def partner_copy(way, hop, h, core):
        piece = gathered.at[2 * source_of(way, hop) + core, pl.ds(h * half, half)]
        return remote(
            piece, piece, p_send.at[0], p_recv.at[shard(way, hop) * 2 + h], ep, partner
        )

    for sub in range(4):
        for way in range(2):
            if sub in subs_of(way, 0):
                gather_copy(way, 0, sub).start()
    for h in range(2):
        partner_copy(0, 0, h, c).start()

    def by_expert(value):
        w = value.shape[1]
        cut_up = value.reshape(sources_half, 2, cap, w)
        return [cut_up[:, e].reshape(part, w) for e in range(2)]

    def expert_in(way, hop, h):
        source = source_of(way, hop)
        partner_copy(way, hop, h, 1 - c).wait_recv()
        at = pl.ds(h * half, half)
        x = jnp.concatenate(
            [gathered[2 * source, at, :], gathered[2 * source + 1, at, :]], axis=1
        ).astype(F32)
        square = jnp.broadcast_to(jnp.sum(x * x, axis=1, keepdims=True), (half, 128))
        squares[h] = square if hop == 0 else squares[h] + square
        depth = x.shape[1]
        deep = pl.ds(pl.multiple_of(source * depth, depth), depth)
        for e, rows_e in enumerate(by_expert(x * gain_ref[source])):
            rows_e = rows_e.astype(BF16)
            for n, w in enumerate((gate_w, up_w)):
                product = nn_dot(rows_e, w[e, deep, :])
                pre[h, e, n] = product if hop == 0 else pre[h, e, n] + product

    for copy in loads[5:]:
        copy.wait()
    spread(1)

    for hop in range(1, far + 1):
        for step in range(4 if hop < far else 2):
            for way in range(2):
                sub = step if hop < far else 2 * way + step
                gather_wait(way, hop, sub)
                if hop < far and sub in subs_of(way, hop):
                    gather_copy(way, hop, sub).start()
            if step % 2 == 1:
                h = step // 2
                for way in range(2):
                    if hop < far:
                        partner_copy(way, hop, h, c).start()
                    else:
                        partner_copy(way, hop, way, c).start()
                for half_at in (h,) if hop < far else (0, 1):
                    expert_in(0, hop - 1, half_at)
                    if hop > 1:
                        expert_in(1, hop - 1, half_at)
    for way in range(2):
        expert_in(way, far, way)

    for h in range(2):
        factor = lax.rsqrt(squares[h] / float(cfg["width"]) + NORM_EPS)
        for e, f in enumerate(by_expert(factor)):
            f = jnp.concatenate([f, f], axis=1)
            gate = jnp.minimum(pre[h, e, 0] * f, CLAMP_LIMIT)
            up = jnp.clip(pre[h, e, 1] * f, -CLAMP_LIMIT, CLAMP_LIMIT)
            hidden[2 * h + e] = ((up + 1.0) * gate * jax.nn.sigmoid(GLU_ALPHA * gate)).astype(
                BF16
            )

    goals = [ring(z, far)]
    for hop in range(1, far):
        goals += [ring(z, far - hop), ring(z, hop - far)]
    goals += [z]

    def goal_of(way, hop):
        return 0 if hop == 0 else 2 * hop - 1 + way

    def down(g):
        wide = pl.ds(pl.multiple_of(goals[g] * 256, 256), 256)
        for he in range(4):
            y = nn_dot(hidden[he], down_w[he % 2, :, wide]).astype(BF16)
            ybuf[0, g, he] = y[:, :128]
            ybuf[1, g, he] = y[:, 128:]
        y_copy(g).start()

    def y_copy(g):
        return remote(
            ybuf.at[1 - c, g], prec.at[g], y_send.at[0], y_recv.at[g], ep, partner
        )

    def sum_copy(way, hop, he):
        to = ring(z, 1) if way == 0 else ring(z, -1)
        at = (way * far + hop) * 4 + he
        return remote(
            rsend.at[at], rrecv.at[at], r_send.at[0], r_recv.at[at], ep, 2 * to + c
        )

    def own_sum(g, he):
        return ybuf[c, g, he].astype(F32) + prec[g, he].astype(F32)

    def arrived_sum(total, way, hop, he):
        if hop > 0 or he // 2 == way:
            sum_copy(way, hop, he).wait_recv()
            total = total + rrecv[(way * far + hop) * 4 + he].astype(F32)
        return total

    down(0)
    for g in (1, 2):
        if far > 1:
            down(g)
    y_copy(0).wait_recv()
    for way in range(2):
        for e in range(2):
            he = 2 * way + e
            rsend[way * far * 4 + he] = own_sum(0, he).astype(BF16)
            sum_copy(way, 0, he).start()
    spread(2)

    def pair(a, places, m, cond):
        def work():
            @pl.when(cond)
            def _():
                attend([held_at(a, b) for b in places], (m,))

        return work

    def own_row(m):
        def work():
            @pl.when(px >= 2)
            def _():
                attend([held_at(0, -1), held_at(0, -2)], (m,))

            @pl.when(px == 1)
            def _():
                attend([held_at(0, -1)], (m,))

        return work

    def own_third():
        @pl.when(px == 3)
        def _():
            attend([held_at(0, -3)], (0, 1))

    up_1, up_2, up_3 = py >= 1, py >= 2, py >= 3
    fillers = [
        own_row(0),
        own_row(1),
        pair(-1, (0, 1), 0, up_1),
        pair(-1, (0, 1), 1, up_1),
        pair(-3, (0, 1), 0, up_3),
        pair(-3, (0, 1), 1, up_3),
        own_third,
        lambda: spread(3),
        pair(-1, (-1, 2), 0, up_1),
        pair(-1, (-1, 2), 1, up_1),
        pair(-3, (-1, 2), 0, up_3),
        pair(-3, (-1, 2), 1, up_3),
        pair(-2, (0, 1), 0, up_2),
        pair(-2, (0, 1), 1, up_2),
        lambda: spread(4),
        pair(-2, (-1, 2), 0, up_2),
        pair(-2, (-1, 2), 1, up_2),
    ]

    def fill(count=1):
        for _ in range(count):
            if fillers:
                fillers.pop(0)()

    for hop in range(1, far):
        for way in range(2):
            y_copy(goal_of(way, hop)).wait_recv()
        for he in range(4):
            fill()
            for way in range(2):
                part_at = he if way == 0 else (he + 2) % 4
                total = arrived_sum(own_sum(goal_of(way, hop), part_at), way, hop - 1, part_at)
                rsend[(way * far + hop) * 4 + part_at] = total.astype(BF16)
                sum_copy(way, hop, part_at).start()
            if he == 1:
                for way in range(2):
                    if hop < far - 1:
                        down(goal_of(way, hop + 1))
                    elif way == 0:
                        down(n_z - 1)
    if far == 1:
        down(n_z - 1)

    last = n_z - 1
    y_copy(last).wait_recv()
    for h in range(2):
        totals = []
        for e in range(2):
            he = 2 * h + e
            fill(2)
            total = own_sum(last, he)
            for way in range(2):
                total = arrived_sum(total, way, far - 1, he)
            totals.append(total.reshape(sources_half, 1, cap, 128))
        back_send[h * half : (h + 1) * half] = (
            jnp.concatenate(totals, axis=1).reshape(half, 128).astype(BF16)
        )
        for s in range(h * sources_half, (h + 1) * sources_half):

            @pl.when(ep != s)
            def _(s=s):
                remote(
                    back_send.at[pl.ds(s * block, block)],
                    back.at[mine],
                    b_sem.at[0],
                    b_sem.at[1],
                    s,
                    tp,
                ).start()

    back[mine, :] = back_send[mine, :]
    fill(len(fillers))

    mix = mix_ref[...]
    for r in range(0, q_rows, tile):
        one, two = pl.ds(r, tile), pl.ds(q_rows + r, tile)
        blend = acc[one, :width] / acc[one, width:] - mix * (acc[two, :width] / acc[two, width:])
        mean = jnp.mean(blend * blend, axis=1, keepdims=True)
        scaled = blend * lax.rsqrt(mean + SUB_EPS)
        attn_ref[one, :] = (scaled * sub_gain_ref[...] * OUT_SCALE).astype(BF16)
    attn_out = pltpu.make_async_copy(attn_ref, attn_hbm, out_sem.at[0])
    attn_out.start()

    remote(arrived, arrived, d_sem.at[0], d_sem.at[1], ep, partner).wait_send()
    for n, buf in enumerate((kbuf, vbuf)):
        whole = buf.at[pl.ds(0, n_ep - 1)]
        remote(whole, whole, kv_send.at[n], kv_recv.at[n, 0], ep, partner).wait_send()
    whole = gathered.at[pl.ds(0, n_z - 1)]
    remote(whole, whole, g_send.at[0], g_recv.at[0], ep, partner).wait_send()
    whole = gathered.at[pl.ds(0, n_z)]
    remote(whole, whole, p_send.at[0], p_recv.at[0], ep, partner).wait_send()
    remote(ybuf.at[0], prec, y_send.at[0], y_recv.at[0], ep, partner).wait_send()
    sent = pl.ds(0, 4 * (n_z - 1))
    remote(rsend.at[sent], rrecv.at[sent], r_send.at[0], r_recv.at[0], ep, partner).wait_send()
    weight = jnp.concatenate(
        [pick_weight_ref[...], jnp.zeros((126, rows), F32)], axis=0
    ).T

    piece = back.at[pl.ds(0, others)]
    remote(piece, piece, b_sem.at[0], b_sem.at[1], ep, partner).wait()
    result = back[...]
    moe_ref[...] = (
        tn_dot(picks[0], result) * weight[:, 0:1] + tn_dot(picks[1], result) * weight[:, 1:2]
    ).astype(BF16)
    moe_out = pltpu.make_async_copy(moe_ref, moe_hbm, out_sem.at[1])
    moe_out.start()
    attn_out.wait()
    moe_out.wait()


def shards(
    queries,
    keys,
    values,
    mix_weight,
    sub_gain,
    tokens,
    routes,
    route_weights,
    expert_gain,
    gate_weight,
    up_weight,
    down_weight,
):
    n_ep, n_tp = lax.axis_size("ep"), lax.axis_size("tp")
    n_z = n_tp // 2
    rows, pick_count = routes.shape
    experts = n_ep * gate_weight.shape[0]
    cap = 3 * rows * pick_count // (2 * experts)
    slots = experts * cap
    part = slots // 4
    q_rows, _, qk_width = queries.shape
    v_width = values.shape[2]
    width = expert_gain.shape[0]
    ff = gate_weight.shape[2]
    cfg = dict(n_ep=n_ep, n_tp=n_tp, cap=cap, rows=rows, width=width)
    dma = pltpu.SemaphoreType.DMA
    vmem = pltpu.VMEM
    anywhere = pl.BlockSpec(memory_space=pl.ANY)
    attn_out, moe_out = pl.pallas_call(
        functools.partial(kernel, cfg),
        name="layer",
        out_shape=(
            jax.ShapeDtypeStruct((q_rows, v_width), BF16),
            jax.ShapeDtypeStruct((rows, tokens.shape[1]), BF16),
        ),
        in_specs=[anywhere] * 12,
        out_specs=(anywhere, anywhere),
        scratch_shapes=[
            vmem((q_rows, qk_width), BF16),
            vmem((1, 1), F32),
            vmem((1, v_width), F32),
            vmem(tokens.shape, BF16),
            vmem((pick_count, rows), jnp.int32),
            vmem((pick_count, rows), F32),
            vmem((n_z, 1, width // n_z), F32),
            vmem(gate_weight.shape, BF16),
            vmem(up_weight.shape, BF16),
            vmem(down_weight.shape, BF16),
            vmem((q_rows, v_width), BF16),
            vmem((rows, tokens.shape[1]), BF16),
            vmem((2 * q_rows, qk_width), BF16),
            vmem((n_ep, q_rows, qk_width), BF16),
            vmem((n_ep, q_rows, v_width), BF16),
            vmem((2 * q_rows, 2 * v_width), F32),
            vmem((2 * q_rows, 128), F32),
            vmem((2, slots, rows), BF16),
            vmem((slots, tokens.shape[1]), BF16),
            vmem((n_tp, slots, tokens.shape[1]), BF16),
            vmem((2, 2, 2, part, ff), F32),
            vmem((2, slots // 2, 128), F32),
            vmem((4, part, ff), BF16),
            vmem((2, n_z, 4, part, 128), BF16),
            vmem((n_z, 4, part, 128), BF16),
            vmem((4 * n_z, part, 128), BF16),
            vmem((4 * n_z, part, 128), BF16),
            vmem((slots, 128), BF16),
            vmem((slots, 128), BF16),
            dma((12,)),
            dma((2,)),
            dma((2,)),
            dma((2, n_ep)),
            dma((2,)),
            dma((1,)),
            dma((4 * n_z,)),
            dma((1,)),
            dma((2 * n_z,)),
            dma((1,)),
            dma((n_z,)),
            dma((1,)),
            dma((4 * n_z,)),
            dma((2,)),
        ],
        compiler_params=pltpu.CompilerParams(
            collective_id=0, has_side_effects=True, vmem_limit_bytes=60 * 1024 * 1024
        ),
    )(
        queries.reshape(q_rows, qk_width),
        keys.reshape(q_rows, qk_width),
        values.reshape(q_rows, v_width),
        mix_weight.reshape(1, 1),
        sub_gain.reshape(1, v_width),
        tokens,
        routes.T,
        route_weights.T,
        expert_gain.reshape(n_z, 1, width // n_z),
        gate_weight,
        up_weight,
        down_weight,
    )
    return attn_out.reshape(q_rows, 1, v_width), moe_out


def solution(mesh):
    return jax.shard_map(
        shards,
        mesh=mesh,
        in_specs=(
            P("ep", "tp", None),
            P("ep", "tp", None),
            P("ep", "tp", None),
            P("tp"),
            P(),
            P("ep", "tp"),
            P("ep", None),
            P("ep", None),
            P(),
            P("ep", None, "tp"),
            P("ep", None, "tp"),
            P("ep", "tp", None),
        ),
        out_specs=(P("ep", "tp", None), P("ep", "tp")),
        check_vma=False,
    )
```

```python
import functools
import math

import jax
import jax.numpy as jnp
from jax import lax
from jax.experimental import pallas as pl
from jax.experimental.pallas import tpu as pltpu
from jax.sharding import PartitionSpec as P

MESH = pl.DeviceIdType.MESH
NEG_FILL = -1e30
SUB_EPS = 1e-05
NORM_EPS = 1e-06
CLAMP_LIMIT = 7.0
GLU_ALPHA = 1.702
OUT_SCALE = 0.8
F32 = jnp.float32
BF16 = jnp.bfloat16


def nt_dot(a, b):
    return lax.dot_general(a, b, (((1,), (1,)), ((), ())), preferred_element_type=F32)


def nn_dot(a, b):
    return jnp.dot(a, b, preferred_element_type=F32)


STAGES = (
    ((), (((0, 0), "x+"), ((0, 0), "x-"), ((0, 0), "y+"), ((0, 0), "y-"))),
    (
        ((0, -1), (0, 1), (-1, 0), (1, 0)),
        (
            ((0, -1), "x+"),
            ((0, -1), "y+"),
            ((0, -1), "y-"),
            ((0, 1), "y+"),
            ((0, 1), "y-"),
            ((-1, 0), "y+"),
        ),
    ),
    (
        ((0, 2), (-1, -1), (1, -1), (-1, 1), (1, 1), (2, 0)),
        (((0, 2), "y+"), ((0, 2), "y-"), ((-1, -1), "y+"), ((1, 1), "y-")),
    ),
    (((-1, 2), (1, 2), (2, -1), (2, 1)), (((1, 2), "y-"),)),
    (((2, 2),), ()),
)
STEP = {"x+": (0, 1), "x-": (0, -1), "y+": (1, 0), "y-": (-1, 0)}
MIRROR = {"x+": "y-", "x-": "y+", "y+": "x-", "y-": "x+"}
SIDE = 4


def kernel(
    cfg,
    q_hbm,
    k_hbm,
    v_hbm,
    mix_hbm,
    sub_gain_hbm,
    tokens_hbm,
    routes_hbm,
    pick_weight_hbm,
    gain_hbm,
    gate_hbm,
    up_hbm,
    down_hbm,
    attn_hbm,
    moe_hbm,
    q_ref,
    mix_ref,
    sub_gain_ref,
    tokens_ref,
    routes_ref,
    pick_weight_ref,
    gain_ref,
    gate_w,
    up_w,
    down_w,
    attn_ref,
    moe_ref,
    qz,
    kbuf,
    vbuf,
    acc,
    row_max,
    picks,
    outgoing,
    gathered,
    pre,
    squares,
    hidden,
    ybuf,
    prec,
    rsend,
    rrecv,
    back_send,
    back,
    in_sem,
    out_sem,
    kv_send,
    kv_recv,
    d_sem,
    g_send,
    g_recv,
    p_send,
    p_recv,
    y_send,
    y_recv,
    r_send,
    r_recv,
    b_sem,
):
    n_ep, n_tp, cap, rows = cfg["n_ep"], cfg["n_tp"], cfg["cap"], cfg["rows"]
    n_z = n_tp // 2
    far = n_z // 2
    block = 2 * cap
    slots = n_ep * block
    half = slots // 2
    sources_half = n_ep // 2
    part = half // 2
    ep = lax.axis_index("ep")
    tp = lax.axis_index("tp")
    z, c = lax.div(tp, 2), lax.rem(tp, 2)
    py, px = lax.div(ep, SIDE), lax.rem(ep, SIDE)
    partner = tp + 1 - 2 * c

    def ring(at, shift):
        return lax.rem(at + shift + 2 * n_z, n_z)

    def remote(src, dst, send_sem, recv_sem, to_ep, to_tp):
        return pltpu.make_async_remote_copy(
            src_ref=src,
            dst_ref=dst,
            send_sem=send_sem,
            recv_sem=recv_sem,
            device_id=(to_ep, to_tp),
            device_id_type=MESH,
        )

    barrier = pltpu.get_barrier_semaphore()
    for off in range(1, n_ep):
        pl.semaphore_signal(
            barrier, inc=1, device_id=(lax.rem(ep + off, n_ep), tp), device_id_type=MESH
        )
    for to in (2 * ring(z, 1) + c, 2 * ring(z, -1) + c, partner):
        pl.semaphore_signal(barrier, inc=1, device_id=(ep, to), device_id_type=MESH)

    loads = [
        pltpu.make_async_copy(src, dst, in_sem.at[i])
        for i, (src, dst) in enumerate(
            (
                (routes_hbm, routes_ref),
                (tokens_hbm, tokens_ref),
                (q_hbm, q_ref),
                (k_hbm, kbuf.at[0]),
                (v_hbm, vbuf.at[0]),
                (gain_hbm, gain_ref),
                (gate_hbm, gate_w),
                (up_hbm, up_w),
                (down_hbm, down_w),
                (mix_hbm, mix_ref),
                (sub_gain_hbm, sub_gain_ref),
                (pick_weight_hbm, pick_weight_ref),
            )
        )
    ]
    for copy in loads:
        copy.start()

    for copy in loads[:2]:
        copy.wait()
    pairs = 2 * rows
    experts = 2 * n_ep
    routes = jnp.concatenate([routes_ref[0:1, :], routes_ref[1:2, :]], axis=1)
    member = (
        lax.broadcasted_iota(jnp.int32, (experts, pairs), 0)
        == jnp.broadcast_to(routes, (experts, pairs))
    ).astype(F32)

    def order(dim):
        at = lax.broadcasted_iota(jnp.int32, (pairs, pairs), dim)
        return jnp.where(at < rows, 2 * at, 2 * (at - rows) + 1)

    earlier = (order(0) < order(1)).astype(F32).astype(BF16)
    rank = nn_dot(member.astype(BF16), earlier)
    first_slot = lax.broadcasted_iota(jnp.int32, (experts, pairs), 0).astype(F32) * float(cap)
    target = jnp.sum(member * (rank + first_slot), axis=0, keepdims=True)
    slot_at = lax.broadcasted_iota(jnp.int32, (slots, rows), 0).astype(F32)
    pick_0 = (slot_at == jnp.broadcast_to(target[:, :rows], (slots, rows))).astype(F32)
    pick_1 = (slot_at == jnp.broadcast_to(target[:, rows:], (slots, rows))).astype(F32)
    out_rows = nn_dot((pick_0 + pick_1).astype(BF16), tokens_ref[...]).astype(BF16)
    outgoing[...] = out_rows
    mine = pl.ds(pl.multiple_of(ep * block, block), block)
    gathered[tp, mine, :] = outgoing[mine, :]

    loads[2].wait()
    q_all = q_ref[...]
    q_rows = q_all.shape[0]
    lane = lax.broadcasted_iota(jnp.int32, q_all.shape, 1)
    zero = jnp.zeros_like(q_all)
    qz[:q_rows] = jnp.where(lane < q_all.shape[1] // 2, q_all, zero)
    qz[q_rows:] = jnp.where(lane >= q_all.shape[1] // 2, q_all, zero)

    pl.semaphore_wait(barrier, n_ep - 1 + 3)

    for off in range(1, n_ep):
        to = lax.rem(ep + off, n_ep)
        remote(
            outgoing.at[pl.ds(pl.multiple_of(to * block, block), block)],
            gathered.at[tp, mine],
            d_sem.at[0],
            d_sem.at[1],
            to,
            tp,
        ).start()
    others = (n_ep - 1) * block

    exponent = (q_ref.shape[1] // 2) ** (-0.5) * math.log2(math.e)
    width = vbuf.shape[2]
    tile = min(256, q_rows)

    def scores_at(r, keys, first):
        scores = nt_dot(qz[pl.ds(r, tile), :], keys)
        if first:
            seen = lax.broadcasted_iota(jnp.int32, scores.shape, 1) <= (
                lax.broadcasted_iota(jnp.int32, scores.shape, 0) + r % q_rows
            )
            scores = jnp.where(seen, scores, NEG_FILL)
        return scores

    def attend(held, maps=(0, 1), first=False):
        keys = jnp.concatenate([kbuf[s] for s in held], axis=0)
        values = jnp.concatenate([vbuf[s] for s in held], axis=0)
        both = jnp.concatenate([values, jnp.ones_like(values)], axis=1)
        at = [m * q_rows + r for m in maps for r in range(0, q_rows, tile)]
        scores = [scores_at(r, keys, first) for r in at]
        tops = [jnp.max(s, axis=1, keepdims=True) for s in scores]
        if first:
            tops = [jnp.broadcast_to(t, (tile, 128)) for t in tops]
        else:
            olds = [row_max[pl.ds(r, tile), :] for r in at]
            tops = [jnp.maximum(o, t) for o, t in zip(olds, tops)]
        weights = [
            jnp.exp2((s - t[:, :1]) * exponent).astype(BF16) for s, t in zip(scores, tops)
        ]
        for i, r in enumerate(at):
            where = pl.ds(r, tile)
            added = nn_dot(weights[i], both)
            if first:
                acc[where, :] = added
            else:
                shrink = jnp.exp2((olds[i] - tops[i]) * exponent)
                acc[where, :] = acc[where, :] * jnp.concatenate([shrink, shrink], axis=1) + added
            row_max[where, :] = tops[i]

    def held_at(a, b):
        return (a % SIDE) * SIDE + b % SIDE

    def spread(stage):
        waits, sends = STAGES[stage]
        for n, buf in enumerate((kbuf, vbuf)):
            for a, b in waits:
                at = held_at(a, b) if n == 0 else held_at(-b, -a)
                remote(
                    buf.at[at], buf.at[at], kv_send.at[n], kv_recv.at[n, at], ep, partner
                ).wait_recv()
        for (a, b), way in sends:
            for n, buf in enumerate((kbuf, vbuf)):
                if n == 1:
                    a, b, way = -b, -a, MIRROR[way]
                dy, dx = STEP[way]
                to = lax.rem(py + dy + SIDE, SIDE) * SIDE + lax.rem(px + dx + SIDE, SIDE)
                at = held_at(a - dy, b - dx)
                remote(
                    buf.at[held_at(a, b)], buf.at[at], kv_send.at[n], kv_recv.at[n, at], to, tp
                ).start()

    for copy in loads[3:5]:
        copy.wait()
    attend((0,), first=True)

    column = jnp.broadcast_to(target, (128, pairs)).T
    slot_on = lax.broadcasted_iota(jnp.int32, (rows, 128), 1).astype(F32)
    for n in range(2):
        at_row = column[n * rows : (n + 1) * rows]
        for s0 in range(0, slots, 128):
            picks[n, :, s0 : s0 + 128] = (slot_on + float(s0) == at_row).astype(F32).astype(BF16)
    arrived = gathered.at[tp, pl.ds(0, others)]
    remote(arrived, arrived, d_sem.at[0], d_sem.at[1], ep, partner).wait_recv()

    cut = half // 2

    def source_of(way, hop):
        return ring(z, -hop) if way == 0 else ring(z, hop)

    def gather_copy(way, hop, sub):
        to = ring(z, 1) if way == 0 else ring(z, -1)
        piece = gathered.at[2 * source_of(way, hop) + c, pl.ds(sub * cut, cut)]
        at = (way * far + hop) * 4 + sub
        return remote(piece, piece, g_send.at[0], g_recv.at[at], ep, 2 * to + c)

    def gather_wait(way, hop, sub):
        piece = gathered.at[2 * source_of(way, hop) + c, pl.ds(sub * cut, cut)]
        at = (way * far + hop - 1) * 4 + sub
        remote(piece, piece, g_send.at[0], g_recv.at[at], ep, partner).wait_recv()

    def subs_of(way, hop):
        return range(4) if hop < far - 1 else range(2 * way, 2 * way + 2)

    def shard(way, hop):
        return 0 if hop == 0 else (2 * hop - 1 + way if hop < far else n_z - 1)

    def partner_copy(way, hop, h, core):
        piece = gathered.at[2 * source_of(way, hop) + core, pl.ds(h * half, half)]
        return remote(
            piece, piece, p_send.at[0], p_recv.at[shard(way, hop) * 2 + h], ep, partner
        )

    for sub in range(4):
        for way in range(2):
            if sub in subs_of(way, 0):
                gather_copy(way, 0, sub).start()
    for h in range(2):
        partner_copy(0, 0, h, c).start()

    def by_expert(value):
        w = value.shape[1]
        cut_up = value.reshape(sources_half, 2, cap, w)
        return [cut_up[:, e].reshape(part, w) for e in range(2)]

    def expert_in(way, hop, h):
        source = source_of(way, hop)
        partner_copy(way, hop, h, 1 - c).wait_recv()
        at = pl.ds(h * half, half)
        x = jnp.concatenate(
            [gathered[2 * source, at, :], gathered[2 * source + 1, at, :]], axis=1
        ).astype(F32)
        square = jnp.broadcast_to(jnp.sum(x * x, axis=1, keepdims=True), (half, 128))
        squares[h] = square if hop == 0 else squares[h] + square
        depth = x.shape[1]
        deep = pl.ds(pl.multiple_of(source * depth, depth), depth)
        for e, rows_e in enumerate(by_expert(x * gain_ref[source])):
            rows_e = rows_e.astype(BF16)
            for n, w in enumerate((gate_w, up_w)):
                product = nn_dot(rows_e, w[e, deep, :])
                pre[h, e, n] = product if hop == 0 else pre[h, e, n] + product

    spread(0)
    for copy in loads[5:]:
        copy.wait()
    for h in range(2):
        expert_in(0, 0, h)

    y_1, y_2, y_3 = py >= 1, py >= 2, py >= 3
    x_1, x_2, x_3 = px >= 1, px >= 2, px >= 3

    def pieces(*cases):
        def work(m):
            taken = None
            for cond, places in cases:
                now = cond if taken is None else jnp.logical_and(cond, jnp.logical_not(taken))

                @pl.when(now)
                def _(places=places):
                    attend([held_at(a, b) for a, b in places], (m,))

                taken = cond if taken is None else jnp.logical_or(taken, cond)

        return [functools.partial(work, 0), functools.partial(work, 1)]

    both_2 = jnp.logical_and(x_2, y_2)
    fillers = [
        *pieces((y_3, ((-1, 0), (1, 0))), (y_1, ((-1, 0),))),
        *pieces((x_3, ((0, -1), (0, 1))), (x_1, ((0, -1),))),
        lambda: spread(2),
        *pieces((y_1, ((-1, -1), (-1, 1)))),
        *pieces((y_3, ((1, -1), (1, 1)))),
        *pieces((both_2, ((0, 2), (2, 0))), (x_2, ((0, 2),)), (y_2, ((2, 0),))),
        lambda: spread(3),
        *pieces((y_3, ((-1, 2), (1, 2))), (y_1, ((-1, 2),))),
        *pieces((y_2, ((2, -1), (2, 1)))),
        lambda: spread(4),
        *pieces((y_2, ((2, 2),))),
    ]

    def fill(count=1):
        for _ in range(count):
            if fillers:
                fillers.pop(0)()

    for hop in range(1, far + 1):
        if hop == min(2, far):
            spread(1)
        for step in range(4 if hop < far else 2):
            for way in range(2):
                sub = step if hop < far else 2 * way + step
                gather_wait(way, hop, sub)
                if hop < far and sub in subs_of(way, hop):
                    gather_copy(way, hop, sub).start()
            if step % 2 == 1:
                h = step // 2
                for way in range(2):
                    partner_copy(way, hop, h if hop < far else way, c).start()
            if step == 0 and hop > 1:
                for way in range(2):
                    expert_in(way, hop - 1, 1)
            if step == 2:
                for way in range(2):
                    expert_in(way, hop, 0)
            if hop in (2, 3) and step % 2 == 1:
                fill()
    for way in range(2):
        expert_in(way, far, way)

    for h in range(2):
        factor = lax.rsqrt(squares[h] / float(cfg["width"]) + NORM_EPS)
        for e, f in enumerate(by_expert(factor)):
            f = jnp.concatenate([f, f], axis=1)
            gate = jnp.minimum(pre[h, e, 0] * f, CLAMP_LIMIT)
            up = jnp.clip(pre[h, e, 1] * f, -CLAMP_LIMIT, CLAMP_LIMIT)
            hidden[2 * h + e] = ((up + 1.0) * gate * jax.nn.sigmoid(GLU_ALPHA * gate)).astype(
                BF16
            )

    goals = [ring(z, far)]
    for hop in range(1, far):
        goals += [ring(z, far - hop), ring(z, hop - far)]
    goals += [z]

    def goal_of(way, hop):
        return 0 if hop == 0 else 2 * hop - 1 + way

    def down(g):
        wide = pl.ds(pl.multiple_of(goals[g] * 256, 256), 256)
        for he in range(4):
            y = nn_dot(hidden[he], down_w[he % 2, :, wide]).astype(BF16)
            ybuf[0, g, he] = y[:, :128]
            ybuf[1, g, he] = y[:, 128:]
        y_copy(g).start()

    def y_copy(g):
        return remote(
            ybuf.at[1 - c, g], prec.at[g], y_send.at[0], y_recv.at[g], ep, partner
        )

    def sum_copy(way, hop, he):
        to = ring(z, 1) if way == 0 else ring(z, -1)
        at = (way * far + hop) * 4 + he
        return remote(
            rsend.at[at], rrecv.at[at], r_send.at[0], r_recv.at[at], ep, 2 * to + c
        )

    def own_sum(g, he):
        return ybuf[c, g, he].astype(F32) + prec[g, he].astype(F32)

    def arrived_sum(total, way, hop, he):
        if hop > 0 or he // 2 == way:
            sum_copy(way, hop, he).wait_recv()
            total = total + rrecv[(way * far + hop) * 4 + he].astype(F32)
        return total

    down(0)
    y_copy(0).wait_recv()
    for way in range(2):
        for e in range(2):
            he = 2 * way + e
            rsend[way * far * 4 + he] = own_sum(0, he).astype(BF16)
            sum_copy(way, 0, he).start()
    for g in (1, 2):
        if far > 1:
            down(g)
    fill()

    for hop in range(1, far):
        for way in range(2):
            y_copy(goal_of(way, hop)).wait_recv()
        for he in range(4):
            if hop > 1 or he > 0:
                fill()
            for way in range(2):
                part_at = he if way == 0 else (he + 2) % 4
                total = arrived_sum(own_sum(goal_of(way, hop), part_at), way, hop - 1, part_at)
                rsend[(way * far + hop) * 4 + part_at] = total.astype(BF16)
                sum_copy(way, hop, part_at).start()
            if he == 1:
                for way in range(2):
                    if hop < far - 1:
                        down(goal_of(way, hop + 1))
                    elif way == 0:
                        down(n_z - 1)
    if far == 1:
        down(n_z - 1)

    last = n_z - 1
    y_copy(last).wait_recv()
    for h in range(2):
        totals = []
        for e in range(2):
            he = 2 * h + e
            fill(2)
            total = own_sum(last, he)
            for way in range(2):
                total = arrived_sum(total, way, far - 1, he)
            totals.append(total.reshape(sources_half, 1, cap, 128))
        back_send[h * half : (h + 1) * half] = (
            jnp.concatenate(totals, axis=1).reshape(half, 128).astype(BF16)
        )
        for s in range(h * sources_half, (h + 1) * sources_half):

            @pl.when(ep != s)
            def _(s=s):
                remote(
                    back_send.at[pl.ds(s * block, block)],
                    back.at[mine],
                    b_sem.at[0],
                    b_sem.at[1],
                    s,
                    tp,
                ).start()

    back[mine, :] = back_send[mine, :]
    fill(len(fillers))

    mix = mix_ref[...]
    for r in range(0, q_rows, tile):
        one, two = pl.ds(r, tile), pl.ds(q_rows + r, tile)
        blend = acc[one, :width] / acc[one, width:] - mix * (acc[two, :width] / acc[two, width:])
        mean = jnp.mean(blend * blend, axis=1, keepdims=True)
        scaled = blend * lax.rsqrt(mean + SUB_EPS)
        attn_ref[one, :] = (scaled * sub_gain_ref[...] * OUT_SCALE).astype(BF16)
    attn_out = pltpu.make_async_copy(attn_ref, attn_hbm, out_sem.at[0])
    attn_out.start()

    remote(arrived, arrived, d_sem.at[0], d_sem.at[1], ep, partner).wait_send()
    for n, buf in enumerate((kbuf, vbuf)):
        whole = buf.at[pl.ds(0, n_ep - 1)]
        remote(whole, whole, kv_send.at[n], kv_recv.at[n, 0], ep, partner).wait_send()
    whole = gathered.at[pl.ds(0, n_z - 1)]
    remote(whole, whole, g_send.at[0], g_recv.at[0], ep, partner).wait_send()
    whole = gathered.at[pl.ds(0, n_z)]
    remote(whole, whole, p_send.at[0], p_recv.at[0], ep, partner).wait_send()
    remote(ybuf.at[0], prec, y_send.at[0], y_recv.at[0], ep, partner).wait_send()
    sent = pl.ds(0, 4 * (n_z - 1))
    remote(rsend.at[sent], rrecv.at[sent], r_send.at[0], r_recv.at[0], ep, partner).wait_send()
    weight = jnp.concatenate(
        [pick_weight_ref[...], jnp.zeros((126, rows), F32)], axis=0
    ).T

    piece = back.at[pl.ds(0, others)]
    remote(piece, piece, b_sem.at[0], b_sem.at[1], ep, partner).wait()
    result = back[...]
    moe_ref[...] = (
        nn_dot(picks[0], result) * weight[:, 0:1] + nn_dot(picks[1], result) * weight[:, 1:2]
    ).astype(BF16)
    moe_out = pltpu.make_async_copy(moe_ref, moe_hbm, out_sem.at[1])
    moe_out.start()
    attn_out.wait()
    moe_out.wait()


def hand_on(attn_in, moe_in, attn_ref, moe_ref):
    attn_ref[...] = attn_in[...]
    moe_ref[...] = moe_in[...]


def shards(
    queries,
    keys,
    values,
    mix_weight,
    sub_gain,
    tokens,
    routes,
    route_weights,
    expert_gain,
    gate_weight,
    up_weight,
    down_weight,
):
    n_ep, n_tp = lax.axis_size("ep"), lax.axis_size("tp")
    n_z = n_tp // 2
    rows, pick_count = routes.shape
    experts = n_ep * gate_weight.shape[0]
    cap = 3 * rows * pick_count // (2 * experts)
    slots = experts * cap
    part = slots // 4
    q_rows, _, qk_width = queries.shape
    v_width = values.shape[2]
    width = expert_gain.shape[0]
    ff = gate_weight.shape[2]
    cfg = dict(n_ep=n_ep, n_tp=n_tp, cap=cap, rows=rows, width=width)
    dma = pltpu.SemaphoreType.DMA
    vmem = pltpu.VMEM
    anywhere = pl.BlockSpec(memory_space=pl.ANY)
    attn_out, moe_out = pl.pallas_call(
        functools.partial(kernel, cfg),
        name="layer",
        out_shape=(
            jax.ShapeDtypeStruct((q_rows, v_width), BF16),
            jax.ShapeDtypeStruct((rows, tokens.shape[1]), BF16),
        ),
        in_specs=[anywhere] * 12,
        out_specs=(anywhere, anywhere),
        scratch_shapes=[
            vmem((q_rows, qk_width), BF16),
            vmem((1, 1), F32),
            vmem((1, v_width), F32),
            vmem(tokens.shape, BF16),
            vmem((pick_count, rows), jnp.int32),
            vmem((pick_count, rows), F32),
            vmem((n_z, 1, width // n_z), F32),
            vmem(gate_weight.shape, BF16),
            vmem(up_weight.shape, BF16),
            vmem(down_weight.shape, BF16),
            vmem((q_rows, v_width), BF16),
            vmem((rows, tokens.shape[1]), BF16),
            vmem((2 * q_rows, qk_width), BF16),
            vmem((n_ep, q_rows, qk_width), BF16),
            vmem((n_ep, q_rows, v_width), BF16),
            vmem((2 * q_rows, 2 * v_width), F32),
            vmem((2 * q_rows, 128), F32),
            vmem((2, rows, slots), BF16),
            vmem((slots, tokens.shape[1]), BF16),
            vmem((n_tp, slots, tokens.shape[1]), BF16),
            vmem((2, 2, 2, part, ff), F32),
            vmem((2, slots // 2, 128), F32),
            vmem((4, part, ff), BF16),
            vmem((2, n_z, 4, part, 128), BF16),
            vmem((n_z, 4, part, 128), BF16),
            vmem((4 * n_z, part, 128), BF16),
            vmem((4 * n_z, part, 128), BF16),
            vmem((slots, 128), BF16),
            vmem((slots, 128), BF16),
            dma((12,)),
            dma((2,)),
            dma((2,)),
            dma((2, n_ep)),
            dma((2,)),
            dma((1,)),
            dma((4 * n_z,)),
            dma((1,)),
            dma((2 * n_z,)),
            dma((1,)),
            dma((n_z,)),
            dma((1,)),
            dma((4 * n_z,)),
            dma((2,)),
        ],
        compiler_params=pltpu.CompilerParams(
            collective_id=0, has_side_effects=True, vmem_limit_bytes=60 * 1024 * 1024
        ),
    )(
        queries.reshape(q_rows, qk_width),
        keys.reshape(q_rows, qk_width),
        values.reshape(q_rows, v_width),
        mix_weight.reshape(1, 1),
        sub_gain.reshape(1, v_width),
        tokens,
        routes.T,
        route_weights.T,
        expert_gain.reshape(n_z, 1, width // n_z),
        gate_weight,
        up_weight,
        down_weight,
    )
    whole = pl.BlockSpec(memory_space=vmem)
    attn_out, moe_out = pl.pallas_call(
        hand_on,
        name="hand_on",
        out_shape=(
            jax.ShapeDtypeStruct(attn_out.shape, BF16),
            jax.ShapeDtypeStruct(moe_out.shape, BF16),
        ),
        in_specs=[whole] * 2,
        out_specs=(whole, whole),
    )(attn_out, moe_out)
    return attn_out.reshape(q_rows, 1, v_width), moe_out


def solution(mesh):
    return jax.shard_map(
        shards,
        mesh=mesh,
        in_specs=(
            P("ep", "tp", None),
            P("ep", "tp", None),
            P("ep", "tp", None),
            P("tp"),
            P(),
            P("ep", "tp"),
            P("ep", None),
            P("ep", None),
            P(),
            P("ep", None, "tp"),
            P("ep", None, "tp"),
            P("ep", "tp", None),
        ),
        out_specs=(P("ep", "tp", None), P("ep", "tp")),
        check_vma=False,
    )
```

```python
import functools
import math

import jax
import jax.numpy as jnp
from jax import lax
from jax.experimental import pallas as pl
from jax.experimental.pallas import tpu as pltpu
from jax.sharding import PartitionSpec as P

MESH = pl.DeviceIdType.MESH
NEG_FILL = -1e30
SUB_EPS = 1e-05
NORM_EPS = 1e-06
CLAMP_LIMIT = 7.0
GLU_ALPHA = 1.702
OUT_SCALE = 0.8
F32 = jnp.float32
BF16 = jnp.bfloat16


def nt_dot(a, b):
    return lax.dot_general(a, b, (((1,), (1,)), ((), ())), preferred_element_type=F32)


def nn_dot(a, b):
    return jnp.dot(a, b, preferred_element_type=F32)


STAGES = (
    ((), (((0, 0), "x+"), ((0, 0), "x-"), ((0, 0), "y+"), ((0, 0), "y-"))),
    (
        ((0, -1), (0, 1), (-1, 0), (1, 0)),
        (
            ((0, -1), "x+"),
            ((0, -1), "y+"),
            ((0, -1), "y-"),
            ((0, 1), "y+"),
            ((0, 1), "y-"),
            ((-1, 0), "y+"),
        ),
    ),
    (
        ((0, 2), (-1, -1), (1, -1), (-1, 1), (1, 1), (2, 0)),
        (((0, 2), "y+"), ((0, 2), "y-"), ((-1, -1), "y+"), ((1, 1), "y-")),
    ),
    (((-1, 2), (1, 2), (2, -1), (2, 1)), (((1, 2), "y-"),)),
    (((2, 2),), ()),
)
STEP = {"x+": (0, 1), "x-": (0, -1), "y+": (1, 0), "y-": (-1, 0)}
MIRROR = {"x+": "y-", "x-": "y+", "y+": "x-", "y-": "x+"}
SIDE = 4
ROW_ORDER = (0, 1, -1, 2)
FAR_FIRST = tuple(sorted(((a, b) for a in range(4) for b in range(4)), key=lambda p: -min(p[0], 4 - p[0]) - min(p[1], 4 - p[1])))[:-1]


def kernel(
    cfg,
    q_hbm,
    k_hbm,
    v_hbm,
    mix_hbm,
    sub_gain_hbm,
    tokens_hbm,
    routes_hbm,
    pick_weight_hbm,
    gain_hbm,
    gate_hbm,
    up_hbm,
    down_hbm,
    attn_hbm,
    moe_hbm,
    q_ref,
    mix_ref,
    sub_gain_ref,
    tokens_ref,
    routes_ref,
    pick_weight_ref,
    gain_ref,
    gate_w,
    up_w,
    down_w,
    attn_ref,
    moe_ref,
    qz,
    kbuf,
    vbuf,
    acc,
    row_max,
    picks,
    outgoing,
    gathered,
    pre,
    squares,
    hidden,
    ybuf,
    prec,
    rsend,
    rrecv,
    back_send,
    back,
    in_sem,
    out_sem,
    kv_send,
    kv_recv,
    d_send,
    d_recv,
    g_send,
    g_recv,
    p_send,
    p_recv,
    y_send,
    y_recv,
    r_send,
    r_recv,
    b_sem,
):
    n_ep, n_tp, cap, rows = cfg["n_ep"], cfg["n_tp"], cfg["cap"], cfg["rows"]
    n_z = n_tp // 2
    far = n_z // 2
    block = 2 * cap
    slots = n_ep * block
    half = slots // 2
    sources_half = n_ep // 2
    part = half // 2
    ep = lax.axis_index("ep")
    tp = lax.axis_index("tp")
    z, c = lax.div(tp, 2), lax.rem(tp, 2)
    py, px = lax.div(ep, SIDE), lax.rem(ep, SIDE)
    partner = tp + 1 - 2 * c

    def ring(at, shift):
        return lax.rem(at + shift + 2 * n_z, n_z)

    def remote(src, dst, send_sem, recv_sem, to_ep, to_tp):
        return pltpu.make_async_remote_copy(
            src_ref=src,
            dst_ref=dst,
            send_sem=send_sem,
            recv_sem=recv_sem,
            device_id=(to_ep, to_tp),
            device_id_type=MESH,
        )

    barrier = pltpu.get_barrier_semaphore()
    def across(dy, dx):
        return lax.rem(py + dy + SIDE, SIDE) * SIDE + lax.rem(px + dx + SIDE, SIDE)

    for dy, dx in FAR_FIRST:
        pl.semaphore_signal(barrier, inc=1, device_id=(across(dy, dx), tp), device_id_type=MESH)
    for to in (2 * ring(z, 1) + c, 2 * ring(z, -1) + c, partner):
        pl.semaphore_signal(barrier, inc=1, device_id=(ep, to), device_id_type=MESH)

    loads = [
        pltpu.make_async_copy(src, dst, in_sem.at[i])
        for i, (src, dst) in enumerate(
            (
                (routes_hbm, routes_ref),
                (tokens_hbm, tokens_ref),
                (q_hbm, q_ref),
                (k_hbm, kbuf.at[0]),
                (v_hbm, vbuf.at[0]),
                (gain_hbm, gain_ref),
                (gate_hbm, gate_w),
                (up_hbm, up_w),
                (down_hbm, down_w),
                (mix_hbm, mix_ref),
                (sub_gain_hbm, sub_gain_ref),
                (pick_weight_hbm, pick_weight_ref),
            )
        )
    ]
    for copy in loads:
        copy.start()

    for copy in loads[:2]:
        copy.wait()
    pairs = 2 * rows
    experts = 2 * n_ep
    routes = jnp.concatenate([routes_ref[0:1, :], routes_ref[1:2, :]], axis=1)
    member = (
        lax.broadcasted_iota(jnp.int32, (experts, pairs), 0)
        == jnp.broadcast_to(routes, (experts, pairs))
    ).astype(F32)

    def order(dim):
        at = lax.broadcasted_iota(jnp.int32, (pairs, pairs), dim)
        return jnp.where(at < rows, 2 * at, 2 * (at - rows) + 1)

    earlier = (order(0) < order(1)).astype(F32).astype(BF16)
    rank = nn_dot(member.astype(BF16), earlier)
    first_slot = lax.broadcasted_iota(jnp.int32, (experts, pairs), 0).astype(F32) * float(cap)
    target = jnp.sum(member * (rank + first_slot), axis=0, keepdims=True)
    slot_at = lax.broadcasted_iota(jnp.int32, (slots, rows), 0).astype(F32)
    pick_0 = (slot_at == jnp.broadcast_to(target[:, :rows], (slots, rows))).astype(F32)
    pick_1 = (slot_at == jnp.broadcast_to(target[:, rows:], (slots, rows))).astype(F32)
    out_rows = nn_dot((pick_0 + pick_1).astype(BF16), tokens_ref[...]).astype(BF16)
    outgoing[...] = out_rows
    mine = pl.ds(pl.multiple_of(ep * block, block), block)
    own = pl.ds(pl.multiple_of(px * block, block), block)
    gathered[tp, own, :] = outgoing[mine, :]

    loads[2].wait()
    q_all = q_ref[...]
    q_rows = q_all.shape[0]
    lane = lax.broadcasted_iota(jnp.int32, q_all.shape, 1)
    zero = jnp.zeros_like(q_all)
    qz[:q_rows] = jnp.where(lane < q_all.shape[1] // 2, q_all, zero)
    qz[q_rows:] = jnp.where(lane >= q_all.shape[1] // 2, q_all, zero)

    pl.semaphore_wait(barrier, n_ep - 1 + 3)

    for group, dy in enumerate(ROW_ORDER):
        for dx in range(SIDE):
            if dy == 0 and dx == 0:
                continue
            to = across(-dy, dx)
            at = pl.multiple_of((group * SIDE + px) * block, block)
            remote(
                outgoing.at[pl.ds(pl.multiple_of(to * block, block), block)],
                gathered.at[tp, pl.ds(at, block)],
                d_send.at[0],
                d_recv.at[group],
                to,
                tp,
            ).start()
    others = (n_ep - 1) * block

    exponent = (q_ref.shape[1] // 2) ** (-0.5) * math.log2(math.e)
    width = vbuf.shape[2]
    tile = min(256, q_rows)

    def scores_at(r, keys, first):
        scores = nt_dot(qz[pl.ds(r, tile), :], keys)
        if first:
            seen = lax.broadcasted_iota(jnp.int32, scores.shape, 1) <= (
                lax.broadcasted_iota(jnp.int32, scores.shape, 0) + r % q_rows
            )
            scores = jnp.where(seen, scores, NEG_FILL)
        return scores

    def attend(held, maps=(0, 1), first=False):
        keys = jnp.concatenate([kbuf[s] for s in held], axis=0)
        values = jnp.concatenate([vbuf[s] for s in held], axis=0)
        both = jnp.concatenate([values, jnp.ones_like(values)], axis=1)
        at = [m * q_rows + r for m in maps for r in range(0, q_rows, tile)]
        scores = [scores_at(r, keys, first) for r in at]
        tops = [jnp.max(s, axis=1, keepdims=True) for s in scores]
        if first:
            tops = [jnp.broadcast_to(t, (tile, 128)) for t in tops]
        else:
            olds = [row_max[pl.ds(r, tile), :] for r in at]
            tops = [jnp.maximum(o, t) for o, t in zip(olds, tops)]
        weights = [
            jnp.exp2((s - jnp.concatenate([t] * (s.shape[1] // 128), axis=1)) * exponent).astype(
                BF16
            )
            for s, t in zip(scores, tops)
        ]
        for i, r in enumerate(at):
            where = pl.ds(r, tile)
            added = nn_dot(weights[i], both)
            if first:
                acc[where, :] = added
            else:
                shrink = jnp.exp2((olds[i] - tops[i]) * exponent)
                acc[where, :] = acc[where, :] * jnp.concatenate([shrink, shrink], axis=1) + added
            row_max[where, :] = tops[i]

    def held_at(a, b):
        return (a % SIDE) * SIDE + b % SIDE

    def spread(stage):
        waits, sends = STAGES[stage]
        if waits:
            all_of = kbuf.at[pl.ds(0, 2 * len(waits))]
            remote(all_of, all_of, kv_send.at[0], kv_recv.at[stage - 1], ep, partner).wait_recv()
        for (a, b), way in sends:
            for n, buf in enumerate((kbuf, vbuf)):
                if n == 1:
                    a, b, way = -b, -a, MIRROR[way]
                dy, dx = STEP[way]
                to = across(dy, dx)
                at = held_at(a - dy, b - dx)
                remote(
                    buf.at[held_at(a, b)], buf.at[at], kv_send.at[n], kv_recv.at[stage], to, tp
                ).start()

    for copy in loads[3:5]:
        copy.wait()
    attend((0,), first=True)

    column = jnp.broadcast_to(target, (128, pairs)).T
    slot_on = lax.broadcasted_iota(jnp.int32, (rows, 128), 1).astype(F32)
    for n in range(2):
        at_row = column[n * rows : (n + 1) * rows]
        for s0 in range(0, slots, 128):
            picks[n, :, s0 : s0 + 128] = (slot_on + float(s0) == at_row).astype(F32).astype(BF16)
    cut = half // 2

    def source_of(way, hop):
        return ring(z, -hop) if way == 0 else ring(z, hop)

    def gather_copy(way, hop, sub):
        to = ring(z, 1) if way == 0 else ring(z, -1)
        piece = gathered.at[2 * source_of(way, hop) + c, pl.ds(sub * cut, cut)]
        at = (way * far + hop) * 4 + sub
        return remote(piece, piece, g_send.at[0], g_recv.at[at], ep, 2 * to + c)

    def gather_wait(way, hop, sub):
        piece = gathered.at[2 * source_of(way, hop) + c, pl.ds(sub * cut, cut)]
        at = (way * far + hop - 1) * 4 + sub
        remote(piece, piece, g_send.at[0], g_recv.at[at], ep, partner).wait_recv()

    def subs_of(way, hop):
        return range(4) if hop < far - 1 else range(2 * way, 2 * way + 2)

    def shard(way, hop):
        return 0 if hop == 0 else (2 * hop - 1 + way if hop < far else n_z - 1)

    def partner_copy(way, hop, h, core):
        piece = gathered.at[2 * source_of(way, hop) + core, pl.ds(h * half, half)]
        return remote(
            piece, piece, p_send.at[0], p_recv.at[shard(way, hop) * 2 + h], ep, partner
        )

    for sub in range(4):
        group = gathered.at[tp, pl.ds(0, (SIDE - 1 if sub == 0 else SIDE) * block)]
        remote(group, group, d_send.at[0], d_recv.at[sub], ep, partner).wait_recv()
        for way in range(2):
            if sub in subs_of(way, 0):
                gather_copy(way, 0, sub).start()
        if sub % 2 == 1:
            partner_copy(0, 0, sub // 2, c).start()

    def by_expert(value):
        w = value.shape[1]
        cut_up = value.reshape(sources_half, 2, cap, w)
        return [cut_up[:, e].reshape(part, w) for e in range(2)]

    def expert_in(way, hop, h):
        source = source_of(way, hop)
        partner_copy(way, hop, h, 1 - c).wait_recv()
        at = pl.ds(h * half, half)
        x = jnp.concatenate(
            [gathered[2 * source, at, :], gathered[2 * source + 1, at, :]], axis=1
        ).astype(F32)
        square = jnp.broadcast_to(jnp.sum(x * x, axis=1, keepdims=True), (half, 128))
        squares[h] = square if hop == 0 else squares[h] + square
        depth = x.shape[1]
        deep = pl.ds(pl.multiple_of(source * depth, depth), depth)
        for e, rows_e in enumerate(by_expert(x * gain_ref[source])):
            rows_e = rows_e.astype(BF16)
            for n, w in enumerate((gate_w, up_w)):
                product = nn_dot(rows_e, w[e, deep, :])
                pre[h, e, n] = product if hop == 0 else pre[h, e, n] + product

    spread(0)
    for copy in loads[5:]:
        copy.wait()
    for h in range(2):
        expert_in(0, 0, h)

    y_1, y_2, y_3 = py >= 1, py >= 2, py >= 3
    x_1, x_2, x_3 = px >= 1, px >= 2, px >= 3

    def pieces(*cases):
        def work(m):
            taken = None
            for cond, places in cases:
                now = cond if taken is None else jnp.logical_and(cond, jnp.logical_not(taken))

                @pl.when(now)
                def _(places=places):
                    attend([held_at(a, b) for a, b in places], (m,))

                taken = cond if taken is None else jnp.logical_or(taken, cond)

        return [functools.partial(work, 0), functools.partial(work, 1)]

    both_2 = jnp.logical_and(x_2, y_2)
    fillers = [
        *pieces((y_3, ((-1, 0), (1, 0))), (y_1, ((-1, 0),))),
        *pieces((x_3, ((0, -1), (0, 1))), (x_1, ((0, -1),))),
        lambda: spread(2),
        *pieces((y_1, ((-1, -1), (-1, 1)))),
        *pieces((y_3, ((1, -1), (1, 1)))),
        *pieces((both_2, ((0, 2), (2, 0))), (x_2, ((0, 2),)), (y_2, ((2, 0),))),
        lambda: spread(3),
        *pieces((y_3, ((-1, 2), (1, 2))), (y_1, ((-1, 2),))),
        *pieces((y_2, ((2, -1), (2, 1)))),
    ]
    last_fillers = [lambda: spread(4), *pieces((y_2, ((2, 2),)))]

    def fill(count=1):
        for _ in range(count):
            if fillers:
                fillers.pop(0)()

    for hop in range(1, far + 1):
        for step in range(4 if hop < far else 2):
            if (hop, step) == (2, 2):
                spread(1)
            for way in range(2):
                sub = step if hop < far else 2 * way + step
                gather_wait(way, hop, sub)
                if hop < far and sub in subs_of(way, hop):
                    gather_copy(way, hop, sub).start()
            if step % 2 == 1:
                h = step // 2
                for way in range(2):
                    partner_copy(way, hop, h if hop < far else way, c).start()
            if step == 0 and hop > 1:
                for way in range(2):
                    expert_in(way, hop - 1, 1)
            if step == 2:
                for way in range(2):
                    expert_in(way, hop, 0)
            if (hop, step) in ((2, 2), (2, 3), (3, 1), (3, 3)):
                fill()
    def activate(h):
        factor = lax.rsqrt(squares[h] / float(cfg["width"]) + NORM_EPS)
        for e, f in enumerate(by_expert(factor)):
            f = jnp.concatenate([f, f], axis=1)
            gate = jnp.minimum(pre[h, e, 0] * f, CLAMP_LIMIT)
            up = jnp.clip(pre[h, e, 1] * f, -CLAMP_LIMIT, CLAMP_LIMIT)
            hidden[2 * h + e] = ((up + 1.0) * gate * jax.nn.sigmoid(GLU_ALPHA * gate)).astype(
                BF16
            )

    goals = [ring(z, far)]
    for hop in range(1, far):
        goals += [ring(z, far - hop), ring(z, hop - far)]
    goals += [z]

    def goal_of(way, hop):
        return 0 if hop == 0 else 2 * hop - 1 + way

    def down(g, halves=(0, 1)):
        wide = pl.ds(pl.multiple_of(goals[g] * 256, 256), 256)
        for h in halves:
            for e in range(2):
                y = nn_dot(hidden[2 * h + e], down_w[e, :, wide]).astype(BF16)
                ybuf[0, g, 2 * h + e] = y[:, :128]
                ybuf[1, g, 2 * h + e] = y[:, 128:]
        y_copy(g, halves).start()

    def y_copy(g, halves=(0, 1)):
        at = pl.ds(2 * halves[0], 2 * len(halves))
        sem = g if halves[0] == 0 else n_z
        return remote(
            ybuf.at[1 - c, g, at], prec.at[g, at], y_send.at[0], y_recv.at[sem], ep, partner
        )

    def sum_copy(way, hop, he):
        to = ring(z, 1) if way == 0 else ring(z, -1)
        at = (way * far + hop) * 4 + he
        return remote(
            rsend.at[at], rrecv.at[at], r_send.at[0], r_recv.at[at], ep, 2 * to + c
        )

    def own_sum(g, he):
        return ybuf[c, g, he].astype(F32) + prec[g, he].astype(F32)

    def arrived_sum(total, way, hop, he):
        if hop > 0 or he // 2 == way:
            sum_copy(way, hop, he).wait_recv()
            total = total + rrecv[(way * far + hop) * 4 + he].astype(F32)
        return total

    for h in range(2):
        expert_in(h, far, h)
        activate(h)
        down(0, (h,))
    for way in range(2):
        y_copy(0, (way,)).wait_recv()
        for e in range(2):
            he = 2 * way + e
            rsend[way * far * 4 + he] = own_sum(0, he).astype(BF16)
            sum_copy(way, 0, he).start()
    for g in (1, 2):
        if far > 1:
            down(g)
    for hop in range(1, far):
        for way in range(2):
            y_copy(goal_of(way, hop)).wait_recv()
        for he in range(4):
            if hop > 1 or he > 0:
                fill()
            for way in range(2):
                part_at = (he + 2) % 4 if way == 0 else he
                total = arrived_sum(own_sum(goal_of(way, hop), part_at), way, hop - 1, part_at)
                rsend[(way * far + hop) * 4 + part_at] = total.astype(BF16)
                sum_copy(way, hop, part_at).start()
            if he == 1:
                for way in range(2):
                    if hop < far - 1:
                        down(goal_of(way, hop + 1))
                    elif way == 0:
                        down(n_z - 1)
    if far == 1:
        down(n_z - 1)

    last = n_z - 1
    y_copy(last).wait_recv()
    for h in range(2):
        totals = []
        for e in range(2):
            he = 2 * h + e
            fill()
            total = own_sum(last, he)
            for way in range(2):
                total = arrived_sum(total, way, far - 1, he)
            totals.append(total.reshape(sources_half, 1, cap, 128))
        back_send[h * half : (h + 1) * half] = (
            jnp.concatenate(totals, axis=1).reshape(half, 128).astype(BF16)
        )
        for p in range(h * sources_half, (h + 1) * sources_half):

            @pl.when(px != p)
            def _(p=p):
                to = lax.rem(py + ROW_ORDER[p // SIDE] + SIDE, SIDE) * SIDE + p % SIDE
                remote(
                    back_send.at[pl.ds(p * block, block)],
                    back.at[mine],
                    b_sem.at[0],
                    b_sem.at[1],
                    to,
                    tp,
                ).start()

    back[mine, :] = back_send[own, :]
    fillers += last_fillers
    fill(len(fillers))

    mix = mix_ref[...]
    for r in range(0, q_rows, tile):
        one, two = pl.ds(r, tile), pl.ds(q_rows + r, tile)
        blend = acc[one, :width] / acc[one, width:] - mix * (acc[two, :width] / acc[two, width:])
        mean = jnp.mean(blend * blend, axis=1, keepdims=True)
        scaled = blend * lax.rsqrt(mean + SUB_EPS)
        attn_ref[one, :] = (scaled * sub_gain_ref[...] * OUT_SCALE).astype(BF16)
    attn_out = pltpu.make_async_copy(attn_ref, attn_hbm, out_sem.at[0])
    attn_out.start()

    sent = outgoing.at[pl.ds(0, others)]
    remote(sent, sent, d_send.at[0], d_recv.at[0], ep, partner).wait_send()
    for n, buf in enumerate((kbuf, vbuf)):
        whole = buf.at[pl.ds(0, n_ep - 1)]
        remote(whole, whole, kv_send.at[n], kv_recv.at[0], ep, partner).wait_send()
    whole = gathered.at[pl.ds(0, n_z - 1)]
    remote(whole, whole, g_send.at[0], g_recv.at[0], ep, partner).wait_send()
    whole = gathered.at[pl.ds(0, n_z)]
    remote(whole, whole, p_send.at[0], p_recv.at[0], ep, partner).wait_send()
    remote(ybuf.at[0], prec, y_send.at[0], y_recv.at[0], ep, partner).wait_send()
    sent = pl.ds(0, 4 * (n_z - 1))
    remote(rsend.at[sent], rrecv.at[sent], r_send.at[0], r_recv.at[0], ep, partner).wait_send()
    weight = jnp.concatenate(
        [pick_weight_ref[...], jnp.zeros((126, rows), F32)], axis=0
    ).T

    piece = back.at[pl.ds(0, others)]
    remote(piece, piece, b_sem.at[0], b_sem.at[1], ep, partner).wait()
    result = back[...]
    moe_ref[...] = (
        nn_dot(picks[0], result) * weight[:, 0:1] + nn_dot(picks[1], result) * weight[:, 1:2]
    ).astype(BF16)
    moe_out = pltpu.make_async_copy(moe_ref, moe_hbm, out_sem.at[1])
    moe_out.start()
    attn_out.wait()
    moe_out.wait()


def hand_on(attn_in, moe_in, attn_ref, moe_ref):
    attn_ref[...] = attn_in[...]
    moe_ref[...] = moe_in[...]


def shards(
    queries,
    keys,
    values,
    mix_weight,
    sub_gain,
    tokens,
    routes,
    route_weights,
    expert_gain,
    gate_weight,
    up_weight,
    down_weight,
):
    n_ep, n_tp = lax.axis_size("ep"), lax.axis_size("tp")
    n_z = n_tp // 2
    rows, pick_count = routes.shape
    experts = n_ep * gate_weight.shape[0]
    cap = 3 * rows * pick_count // (2 * experts)
    slots = experts * cap
    part = slots // 4
    q_rows, _, qk_width = queries.shape
    v_width = values.shape[2]
    width = expert_gain.shape[0]
    ff = gate_weight.shape[2]
    cfg = dict(n_ep=n_ep, n_tp=n_tp, cap=cap, rows=rows, width=width)
    dma = pltpu.SemaphoreType.DMA
    vmem = pltpu.VMEM
    anywhere = pl.BlockSpec(memory_space=pl.ANY)
    attn_out, moe_out = pl.pallas_call(
        functools.partial(kernel, cfg),
        name="layer",
        out_shape=(
            jax.ShapeDtypeStruct((q_rows, v_width), BF16),
            jax.ShapeDtypeStruct((rows, tokens.shape[1]), BF16),
        ),
        in_specs=[anywhere] * 12,
        out_specs=(anywhere, anywhere),
        scratch_shapes=[
            vmem((q_rows, qk_width), BF16),
            vmem((1, 1), F32),
            vmem((1, v_width), F32),
            vmem(tokens.shape, BF16),
            vmem((pick_count, rows), jnp.int32),
            vmem((pick_count, rows), F32),
            vmem((n_z, 1, width // n_z), F32),
            vmem(gate_weight.shape, BF16),
            vmem(up_weight.shape, BF16),
            vmem(down_weight.shape, BF16),
            vmem((q_rows, v_width), BF16),
            vmem((rows, tokens.shape[1]), BF16),
            vmem((2 * q_rows, qk_width), BF16),
            vmem((n_ep, q_rows, qk_width), BF16),
            vmem((n_ep, q_rows, v_width), BF16),
            vmem((2 * q_rows, 2 * v_width), F32),
            vmem((2 * q_rows, 128), F32),
            vmem((2, rows, slots), BF16),
            vmem((slots, tokens.shape[1]), BF16),
            vmem((n_tp, slots, tokens.shape[1]), BF16),
            vmem((2, 2, 2, part, ff), F32),
            vmem((2, slots // 2, 128), F32),
            vmem((4, part, ff), BF16),
            vmem((2, n_z, 4, part, 128), BF16),
            vmem((n_z, 4, part, 128), BF16),
            vmem((4 * n_z, part, 128), BF16),
            vmem((4 * n_z, part, 128), BF16),
            vmem((slots, 128), BF16),
            vmem((slots, 128), BF16),
            dma((12,)),
            dma((2,)),
            dma((2,)),
            dma((len(STAGES) - 1,)),
            dma((1,)),
            dma((SIDE,)),
            dma((1,)),
            dma((4 * n_z,)),
            dma((1,)),
            dma((2 * n_z,)),
            dma((1,)),
            dma((n_z + 1,)),
            dma((1,)),
            dma((4 * n_z,)),
            dma((2,)),
        ],
        compiler_params=pltpu.CompilerParams(
            collective_id=0, has_side_effects=True, vmem_limit_bytes=60 * 1024 * 1024
        ),
    )(
        queries.reshape(q_rows, qk_width),
        keys.reshape(q_rows, qk_width),
        values.reshape(q_rows, v_width),
        mix_weight.reshape(1, 1),
        sub_gain.reshape(1, v_width),
        tokens,
        routes.T,
        route_weights.T,
        expert_gain.reshape(n_z, 1, width // n_z),
        gate_weight,
        up_weight,
        down_weight,
    )
    whole = pl.BlockSpec(memory_space=vmem)
    attn_out, moe_out = pl.pallas_call(
        hand_on,
        name="hand_on",
        out_shape=(
            jax.ShapeDtypeStruct(attn_out.shape, BF16),
            jax.ShapeDtypeStruct(moe_out.shape, BF16),
        ),
        in_specs=[whole] * 2,
        out_specs=(whole, whole),
    )(attn_out, moe_out)
    return attn_out.reshape(q_rows, 1, v_width), moe_out


def solution(mesh):
    return jax.shard_map(
        shards,
        mesh=mesh,
        in_specs=(
            P("ep", "tp", None),
            P("ep", "tp", None),
            P("ep", "tp", None),
            P("tp"),
            P(),
            P("ep", "tp"),
            P("ep", None),
            P("ep", None),
            P(),
            P("ep", None, "tp"),
            P("ep", None, "tp"),
            P("ep", "tp", None),
        ),
        out_specs=(P("ep", "tp", None), P("ep", "tp")),
        check_vma=False,
    )
```

```python
import functools
import math

import jax
import jax.numpy as jnp
from jax import lax
from jax.experimental import pallas as pl
from jax.experimental.pallas import tpu as pltpu
from jax.sharding import PartitionSpec as P

MESH = pl.DeviceIdType.MESH
NEG_FILL = -1e30
SUB_EPS = 1e-05
NORM_EPS = 1e-06
CLAMP_LIMIT = 7.0
GLU_ALPHA = 1.702
OUT_SCALE = 0.8
F32 = jnp.float32
BF16 = jnp.bfloat16


def nt_dot(a, b):
    return lax.dot_general(a, b, (((1,), (1,)), ((), ())), preferred_element_type=F32)


def nn_dot(a, b):
    return jnp.dot(a, b, preferred_element_type=F32)


STAGES = (
    ((), (((0, 0), "x+"), ((0, 0), "x-"), ((0, 0), "y+"), ((0, 0), "y-"))),
    (
        ((0, -1), (0, 1), (-1, 0), (1, 0)),
        (
            ((0, -1), "x+"),
            ((0, -1), "y+"),
            ((0, -1), "y-"),
            ((0, 1), "y+"),
            ((0, 1), "y-"),
            ((-1, 0), "y+"),
        ),
    ),
    (
        ((0, 2), (-1, -1), (1, -1), (-1, 1), (1, 1), (2, 0)),
        (((0, 2), "y+"), ((0, 2), "y-"), ((-1, -1), "y+"), ((1, 1), "y-")),
    ),
    (((-1, 2), (1, 2), (2, -1), (2, 1)), (((1, 2), "y-"),)),
    (((2, 2),), ()),
)
STEP = {"x+": (0, 1), "x-": (0, -1), "y+": (1, 0), "y-": (-1, 0)}
MIRROR = {"x+": "y-", "x-": "y+", "y+": "x-", "y-": "x+"}
SIDE = 4
ROW_ORDER = (0, 1, -1, 2)
FAR_FIRST = tuple(sorted(((a, b) for a in range(4) for b in range(4)), key=lambda p: -min(p[0], 4 - p[0]) - min(p[1], 4 - p[1])))[:-1]


def kernel(
    cfg,
    q_hbm,
    k_hbm,
    v_hbm,
    mix_hbm,
    sub_gain_hbm,
    tokens_hbm,
    routes_hbm,
    pick_weight_hbm,
    gain_hbm,
    gate_hbm,
    up_hbm,
    down_hbm,
    attn_hbm,
    moe_hbm,
    q_ref,
    mix_ref,
    sub_gain_ref,
    tokens_ref,
    routes_ref,
    pick_weight_ref,
    gain_ref,
    gate_w,
    up_w,
    down_w,
    attn_ref,
    moe_ref,
    qz,
    kbuf,
    vbuf,
    acc,
    row_max,
    picks,
    outgoing,
    gathered,
    pre,
    squares,
    hidden,
    ybuf,
    prec,
    rsend,
    rrecv,
    back_send,
    back,
    in_sem,
    out_sem,
    kv_send,
    kv_recv,
    d_send,
    d_recv,
    g_send,
    g_recv,
    p_send,
    p_recv,
    y_send,
    y_recv,
    r_send,
    r_recv,
    b_sem,
):
    n_ep, n_tp, cap, rows = cfg["n_ep"], cfg["n_tp"], cfg["cap"], cfg["rows"]
    n_z = n_tp // 2
    far = n_z // 2
    block = 2 * cap
    slots = n_ep * block
    half = slots // 2
    sources_half = n_ep // 2
    part = half // 2
    ep = lax.axis_index("ep")
    tp = lax.axis_index("tp")
    z, c = lax.div(tp, 2), lax.rem(tp, 2)
    py, px = lax.div(ep, SIDE), lax.rem(ep, SIDE)
    partner = tp + 1 - 2 * c

    def ring(at, shift):
        return lax.rem(at + shift + 2 * n_z, n_z)

    def remote(src, dst, send_sem, recv_sem, to_ep, to_tp):
        return pltpu.make_async_remote_copy(
            src_ref=src,
            dst_ref=dst,
            send_sem=send_sem,
            recv_sem=recv_sem,
            device_id=(to_ep, to_tp),
            device_id_type=MESH,
        )

    barrier = pltpu.get_barrier_semaphore()
    def across(dy, dx):
        return lax.rem(py + dy + SIDE, SIDE) * SIDE + lax.rem(px + dx + SIDE, SIDE)

    for dy, dx in FAR_FIRST:
        pl.semaphore_signal(barrier, inc=1, device_id=(across(dy, dx), tp), device_id_type=MESH)
    for to in (2 * ring(z, 1) + c, 2 * ring(z, -1) + c, partner):
        pl.semaphore_signal(barrier, inc=1, device_id=(ep, to), device_id_type=MESH)

    loads = [
        pltpu.make_async_copy(src, dst, in_sem.at[i])
        for i, (src, dst) in enumerate(
            (
                (routes_hbm, routes_ref),
                (tokens_hbm, tokens_ref),
                (q_hbm, q_ref),
                (k_hbm, kbuf.at[0]),
                (v_hbm, vbuf.at[0]),
                (gain_hbm, gain_ref),
                (gate_hbm, gate_w),
                (up_hbm, up_w),
                (down_hbm, down_w),
                (mix_hbm, mix_ref),
                (sub_gain_hbm, sub_gain_ref),
                (pick_weight_hbm, pick_weight_ref),
            )
        )
    ]
    for copy in loads:
        copy.start()

    for copy in loads[:2]:
        copy.wait()
    pairs = 2 * rows
    experts = 2 * n_ep
    routes = jnp.concatenate([routes_ref[0:1, :], routes_ref[1:2, :]], axis=1)
    member = (
        lax.broadcasted_iota(jnp.int32, (experts, pairs), 0)
        == jnp.broadcast_to(routes, (experts, pairs))
    ).astype(F32)

    def order(dim):
        at = lax.broadcasted_iota(jnp.int32, (pairs, pairs), dim)
        return jnp.where(at < rows, 2 * at, 2 * (at - rows) + 1)

    earlier = (order(0) < order(1)).astype(F32).astype(BF16)
    rank = nn_dot(member.astype(BF16), earlier)
    first_slot = lax.broadcasted_iota(jnp.int32, (experts, pairs), 0).astype(F32) * float(cap)
    target = jnp.sum(member * (rank + first_slot), axis=0, keepdims=True)
    slot_at = lax.broadcasted_iota(jnp.int32, (slots, rows), 0).astype(F32)
    pick_0 = (slot_at == jnp.broadcast_to(target[:, :rows], (slots, rows))).astype(F32)
    pick_1 = (slot_at == jnp.broadcast_to(target[:, rows:], (slots, rows))).astype(F32)
    out_rows = nn_dot((pick_0 + pick_1).astype(BF16), tokens_ref[...]).astype(BF16)
    outgoing[...] = out_rows
    mine = pl.ds(pl.multiple_of(ep * block, block), block)
    own = pl.ds(pl.multiple_of(px * block, block), block)
    gathered[tp, own, :] = outgoing[mine, :]

    loads[2].wait()
    q_all = q_ref[...]
    q_rows = q_all.shape[0]
    lane = lax.broadcasted_iota(jnp.int32, q_all.shape, 1)
    zero = jnp.zeros_like(q_all)
    qz[:q_rows] = jnp.where(lane < q_all.shape[1] // 2, q_all, zero)
    qz[q_rows:] = jnp.where(lane >= q_all.shape[1] // 2, q_all, zero)

    pl.semaphore_wait(barrier, n_ep - 1 + 3)

    for group, dy in enumerate(ROW_ORDER):
        for dx in range(SIDE):
            if dy == 0 and dx == 0:
                continue
            to = across(-dy, dx)
            at = pl.multiple_of((group * SIDE + px) * block, block)
            remote(
                outgoing.at[pl.ds(pl.multiple_of(to * block, block), block)],
                gathered.at[tp, pl.ds(at, block)],
                d_send.at[0],
                d_recv.at[group],
                to,
                tp,
            ).start()
    others = (n_ep - 1) * block

    exponent = (q_ref.shape[1] // 2) ** (-0.5) * math.log2(math.e)
    width = vbuf.shape[2]
    tile = min(256, q_rows)

    def scores_at(r, keys, first):
        scores = nt_dot(qz[pl.ds(r, tile), :], keys)
        if first:
            seen = lax.broadcasted_iota(jnp.int32, scores.shape, 1) <= (
                lax.broadcasted_iota(jnp.int32, scores.shape, 0) + r % q_rows
            )
            scores = jnp.where(seen, scores, NEG_FILL)
        return scores

    def attend(held, maps=(0, 1), first=False):
        keys = jnp.concatenate([kbuf[s] for s in held], axis=0)
        values = jnp.concatenate([vbuf[s] for s in held], axis=0)
        both = jnp.concatenate([values, jnp.ones_like(values)], axis=1)
        at = [m * q_rows + r for m in maps for r in range(0, q_rows, tile)]
        scores = [scores_at(r, keys, first) for r in at]
        tops = [jnp.max(s, axis=1, keepdims=True) for s in scores]
        if first:
            tops = [jnp.broadcast_to(t, (tile, 128)) for t in tops]
        else:
            olds = [row_max[pl.ds(r, tile), :] for r in at]
            tops = [jnp.maximum(o, t) for o, t in zip(olds, tops)]
        weights = [
            jnp.exp2((s - jnp.concatenate([t] * (s.shape[1] // 128), axis=1)) * exponent).astype(
                BF16
            )
            for s, t in zip(scores, tops)
        ]
        for i, r in enumerate(at):
            where = pl.ds(r, tile)
            added = nn_dot(weights[i], both)
            if first:
                acc[where, :] = added
            else:
                shrink = jnp.exp2((olds[i] - tops[i]) * exponent)
                acc[where, :] = acc[where, :] * jnp.concatenate([shrink, shrink], axis=1) + added
            row_max[where, :] = tops[i]

    def held_at(a, b):
        return (a % SIDE) * SIDE + b % SIDE

    def spread(stage):
        waits, sends = STAGES[stage]
        if waits:
            all_of = kbuf.at[pl.ds(0, 2 * len(waits))]
            remote(all_of, all_of, kv_send.at[0], kv_recv.at[stage - 1], ep, partner).wait_recv()
        for (a, b), way in sends:
            for n, buf in enumerate((kbuf, vbuf)):
                if n == 1:
                    a, b, way = -b, -a, MIRROR[way]
                dy, dx = STEP[way]
                to = across(dy, dx)
                at = held_at(a - dy, b - dx)
                remote(
                    buf.at[held_at(a, b)], buf.at[at], kv_send.at[n], kv_recv.at[stage], to, tp
                ).start()

    for copy in loads[3:5]:
        copy.wait()
    attend((0,), first=True)

    column = jnp.broadcast_to(target, (128, pairs)).T
    slot_on = lax.broadcasted_iota(jnp.int32, (rows, 128), 1).astype(F32)
    for n in range(2):
        at_row = column[n * rows : (n + 1) * rows]
        for s0 in range(0, slots, 128):
            picks[n, :, s0 : s0 + 128] = (slot_on + float(s0) == at_row).astype(F32).astype(BF16)
    cut = half // 2

    def source_of(way, hop):
        return ring(z, -hop) if way == 0 else ring(z, hop)

    def gather_copy(way, hop, sub):
        to = ring(z, 1) if way == 0 else ring(z, -1)
        piece = gathered.at[2 * source_of(way, hop) + c, pl.ds(sub * cut, cut)]
        at = (way * far + hop) * 4 + sub
        return remote(piece, piece, g_send.at[0], g_recv.at[at], ep, 2 * to + c)

    def gather_wait(way, hop, sub):
        piece = gathered.at[2 * source_of(way, hop) + c, pl.ds(sub * cut, cut)]
        at = (way * far + hop - 1) * 4 + sub
        remote(piece, piece, g_send.at[0], g_recv.at[at], ep, partner).wait_recv()

    def subs_of(way, hop):
        return range(4) if hop < far - 1 else range(way, 4, 2)

    def sub_at(way, step):
        return step if way == 0 else step // 2 * 2 + 1 - step % 2

    def shard(way, hop):
        return 0 if hop == 0 else (2 * hop - 1 + way if hop < far else n_z - 1)

    def partner_copy(way, hop, h, core):
        piece = gathered.at[2 * source_of(way, hop) + core, pl.ds(h * half, half)]
        return remote(
            piece, piece, p_send.at[0], p_recv.at[shard(way, hop) * 2 + h], ep, partner
        )

    for sub in range(4):
        group = gathered.at[tp, pl.ds(0, (SIDE - 1 if sub == 0 else SIDE) * block)]
        remote(group, group, d_send.at[0], d_recv.at[sub], ep, partner).wait_recv()
        if sub % 2 == 0:
            gather_copy(0, 0, sub).start()
        else:
            gather_copy(1, 0, sub).start()
            gather_copy(0, 0, sub).start()
            gather_copy(1, 0, sub - 1).start()
            partner_copy(0, 0, sub // 2, c).start()

    def by_expert(value):
        w = value.shape[1]
        cut_up = value.reshape(sources_half, 2, cap, w)
        return [cut_up[:, e].reshape(part, w) for e in range(2)]

    def expert_in(way, hop, h):
        source = source_of(way, hop)
        partner_copy(way, hop, h, 1 - c).wait_recv()
        at = pl.ds(h * half, half)
        x = jnp.concatenate(
            [gathered[2 * source, at, :], gathered[2 * source + 1, at, :]], axis=1
        ).astype(F32)
        square = jnp.broadcast_to(jnp.sum(x * x, axis=1, keepdims=True), (half, 128))
        squares[h] = square if hop == 0 else squares[h] + square
        depth = x.shape[1]
        deep = pl.ds(pl.multiple_of(source * depth, depth), depth)
        for e, rows_e in enumerate(by_expert(x * gain_ref[source])):
            rows_e = rows_e.astype(BF16)
            for n, w in enumerate((gate_w, up_w)):
                product = nn_dot(rows_e, w[e, deep, :])
                pre[h, e, n] = product if hop == 0 else pre[h, e, n] + product

    spread(0)
    for copy in loads[5:]:
        copy.wait()
    for h in range(2):
        expert_in(0, 0, h)

    y_1, y_2, y_3 = py >= 1, py >= 2, py >= 3
    x_1, x_2, x_3 = px >= 1, px >= 2, px >= 3

    def pieces(*cases):
        def work(m):
            taken = None
            for cond, places in cases:
                now = cond if taken is None else jnp.logical_and(cond, jnp.logical_not(taken))

                @pl.when(now)
                def _(places=places):
                    attend([held_at(a, b) for a, b in places], (m,))

                taken = cond if taken is None else jnp.logical_or(taken, cond)

        return [functools.partial(work, 0), functools.partial(work, 1)]

    both_2 = jnp.logical_and(x_2, y_2)
    fillers = [
        *pieces((y_3, ((-1, 0), (1, 0))), (y_1, ((-1, 0),))),
        *pieces((x_3, ((0, -1), (0, 1))), (x_1, ((0, -1),))),
        lambda: spread(2),
        *pieces((y_1, ((-1, -1), (-1, 1)))),
        *pieces((y_3, ((1, -1), (1, 1)))),
        *pieces((both_2, ((0, 2), (2, 0))), (x_2, ((0, 2),)), (y_2, ((2, 0),))),
        lambda: None,
        lambda: None,
        lambda: spread(3),
        *pieces((y_3, ((-1, 2), (1, 2))), (y_1, ((-1, 2),))),
        *pieces((y_2, ((2, -1), (2, 1)))),
    ]
    last_fillers = [lambda: spread(4), *pieces((y_2, ((2, 2),)))]

    def fill(count=1):
        for _ in range(count):
            if fillers:
                fillers.pop(0)()

    def activate(h):
        factor = lax.rsqrt(squares[h] / float(cfg["width"]) + NORM_EPS)
        for e, f in enumerate(by_expert(factor)):
            f = jnp.concatenate([f, f], axis=1)
            gate = jnp.minimum(pre[h, e, 0] * f, CLAMP_LIMIT)
            up = jnp.clip(pre[h, e, 1] * f, -CLAMP_LIMIT, CLAMP_LIMIT)
            hidden[2 * h + e] = ((up + 1.0) * gate * jax.nn.sigmoid(GLU_ALPHA * gate)).astype(
                BF16
            )

    for hop in range(1, far):
        for step in range(4):
            if (hop, step) == (2, 2):
                spread(1)
            for way in range(2):
                sub = sub_at(way, step)
                gather_wait(way, hop, sub)
                if sub in subs_of(way, hop):
                    gather_copy(way, hop, sub).start()
            if step % 2 == 1:
                for way in range(2):
                    partner_copy(way, hop, step // 2, c).start()
            if step == 0 and hop > 1:
                for way in range(2):
                    expert_in(way, hop - 1, 1)
            if step == 2:
                for way in range(2):
                    expert_in(way, hop, 0)
            if (hop, step) in ((2, 2), (2, 3), (3, 1), (3, 3)):
                fill()

    def gather_last(h):
        for way in range(2):
            gather_wait(way, far, 2 * h + way)
        partner_copy(0, far, h, c).start()

    goals = [ring(z, far)]
    for hop in range(1, far):
        goals += [ring(z, far - hop), ring(z, hop - far)]
    goals += [z]

    def goal_of(way, hop):
        return 0 if hop == 0 else 2 * hop - 1 + way

    def down(g, h):
        wide = pl.ds(pl.multiple_of(goals[g] * 256, 256), 256)
        for e in range(2):
            y = nn_dot(hidden[2 * h + e], down_w[e, :, wide]).astype(BF16)
            ybuf[0, g, 2 * h + e] = y[:, :128]
            ybuf[1, g, 2 * h + e] = y[:, 128:]
        y_copy(g, h).start()

    def y_copy(g, h):
        at = pl.ds(2 * h, 2)
        return remote(
            ybuf.at[1 - c, g, at],
            prec.at[g, at],
            y_send.at[0],
            y_recv.at[2 * g + h],
            ep,
            partner,
        )

    def sum_copy(way, hop, he):
        to = ring(z, 1) if way == 0 else ring(z, -1)
        at = (way * far + hop) * 4 + he
        return remote(
            rsend.at[at], rrecv.at[at], r_send.at[0], r_recv.at[at], ep, 2 * to + c
        )

    def own_sum(g, he):
        return ybuf[c, g, he].astype(F32) + prec[g, he].astype(F32)

    def arrived_sum(total, way, hop, he):
        if hop > 0 or he % 2 == way:
            sum_copy(way, hop, he).wait_recv()
            total = total + rrecv[(way * far + hop) * 4 + he].astype(F32)
        return total

    def pass_on(way, hop, he):
        total = own_sum(goal_of(way, hop), he)
        if hop > 0:
            total = arrived_sum(total, way, hop - 1, he)
        rsend[(way * far + hop) * 4 + he] = total.astype(BF16)
        sum_copy(way, hop, he).start()

    def begin(h):
        y_copy(0, h).wait_recv()
        for way in range(2):
            pass_on(way, 0, 2 * h + way)

    def fresh(h):
        for way in range(2):
            y_copy(goal_of(way, 1), h).wait_recv()
            pass_on(way, 1, 2 * h + 1 - way)

    def finish_expert(h):
        expert_in(0, far, h)
        activate(h)
        down(0, h)

    gather_last(0)
    for way in range(2):
        expert_in(way, far - 1, 1)
    finish_expert(0)
    for g in (1, 2):
        down(g, 0)
    gather_last(1)
    begin(0)
    finish_expert(1)
    fresh(0)
    for g in (1, 2):
        down(g, 1)
    begin(1)
    fresh(1)
    for g in (3, 4):
        for h in range(2):
            down(g, h)

    for hop in range(1, far):
        if hop > 1:
            for way in range(2):
                for h in range(2):
                    y_copy(goal_of(way, hop), h).wait_recv()
        for step in range(2 if hop == 1 else 0, 4):
            fill()
            for way in range(2):
                e = 1 - way if step < 2 else way
                pass_on(way, hop, step % 2 * 2 + e)
            if step == 2:
                for g in {1: (), 2: (5, 6), 3: (7,)}[hop]:
                    for h in range(2):
                        down(g, h)

    last = n_z - 1
    for h in range(2):
        y_copy(last, h).wait_recv()
    for h in range(2):
        totals = []
        for e in range(2):
            he = 2 * h + e
            if he == 0:
                fill(3)
            total = own_sum(last, he)
            for way in range(2):
                total = arrived_sum(total, way, far - 1, he)
            totals.append(total.reshape(sources_half, 1, cap, 128))
        back_send[h * half : (h + 1) * half] = (
            jnp.concatenate(totals, axis=1).reshape(half, 128).astype(BF16)
        )
        for p in range(h * sources_half, (h + 1) * sources_half):

            @pl.when(px != p)
            def _(p=p):
                to = lax.rem(py + ROW_ORDER[p // SIDE] + SIDE, SIDE) * SIDE + p % SIDE
                remote(
                    back_send.at[pl.ds(p * block, block)],
                    back.at[mine],
                    b_sem.at[0],
                    b_sem.at[1],
                    to,
                    tp,
                ).start()

    back[mine, :] = back_send[own, :]
    fillers += last_fillers
    fill(len(fillers))

    mix = mix_ref[...]
    for r in range(0, q_rows, tile):
        one, two = pl.ds(r, tile), pl.ds(q_rows + r, tile)
        blend = acc[one, :width] / acc[one, width:] - mix * (acc[two, :width] / acc[two, width:])
        mean = jnp.mean(blend * blend, axis=1, keepdims=True)
        scaled = blend * lax.rsqrt(mean + SUB_EPS)
        attn_ref[one, :] = (scaled * sub_gain_ref[...] * OUT_SCALE).astype(BF16)
    attn_out = pltpu.make_async_copy(attn_ref, attn_hbm, out_sem.at[0])
    attn_out.start()

    sent = outgoing.at[pl.ds(0, others)]
    remote(sent, sent, d_send.at[0], d_recv.at[0], ep, partner).wait_send()
    for n, buf in enumerate((kbuf, vbuf)):
        whole = buf.at[pl.ds(0, n_ep - 1)]
        remote(whole, whole, kv_send.at[n], kv_recv.at[0], ep, partner).wait_send()
    whole = gathered.at[pl.ds(0, n_z - 1)]
    remote(whole, whole, g_send.at[0], g_recv.at[0], ep, partner).wait_send()
    whole = gathered.at[pl.ds(0, n_z)]
    remote(whole, whole, p_send.at[0], p_recv.at[0], ep, partner).wait_send()
    remote(ybuf.at[0], prec, y_send.at[0], y_recv.at[0], ep, partner).wait_send()
    sent = pl.ds(0, 4 * (n_z - 1))
    remote(rsend.at[sent], rrecv.at[sent], r_send.at[0], r_recv.at[0], ep, partner).wait_send()
    weight = jnp.concatenate(
        [pick_weight_ref[...], jnp.zeros((126, rows), F32)], axis=0
    ).T

    piece = back.at[pl.ds(0, others)]
    remote(piece, piece, b_sem.at[0], b_sem.at[1], ep, partner).wait()
    result = back[...]
    moe_ref[...] = (
        nn_dot(picks[0], result) * weight[:, 0:1] + nn_dot(picks[1], result) * weight[:, 1:2]
    ).astype(BF16)
    moe_out = pltpu.make_async_copy(moe_ref, moe_hbm, out_sem.at[1])
    moe_out.start()
    attn_out.wait()
    moe_out.wait()


def hand_on(attn_in, moe_in, attn_ref, moe_ref):
    attn_ref[...] = attn_in[...]
    moe_ref[...] = moe_in[...]


def shards(
    queries,
    keys,
    values,
    mix_weight,
    sub_gain,
    tokens,
    routes,
    route_weights,
    expert_gain,
    gate_weight,
    up_weight,
    down_weight,
):
    n_ep, n_tp = lax.axis_size("ep"), lax.axis_size("tp")
    n_z = n_tp // 2
    rows, pick_count = routes.shape
    experts = n_ep * gate_weight.shape[0]
    cap = 3 * rows * pick_count // (2 * experts)
    slots = experts * cap
    part = slots // 4
    q_rows, _, qk_width = queries.shape
    v_width = values.shape[2]
    width = expert_gain.shape[0]
    ff = gate_weight.shape[2]
    cfg = dict(n_ep=n_ep, n_tp=n_tp, cap=cap, rows=rows, width=width)
    dma = pltpu.SemaphoreType.DMA
    vmem = pltpu.VMEM
    anywhere = pl.BlockSpec(memory_space=pl.ANY)
    attn_out, moe_out = pl.pallas_call(
        functools.partial(kernel, cfg),
        name="layer",
        out_shape=(
            jax.ShapeDtypeStruct((q_rows, v_width), BF16),
            jax.ShapeDtypeStruct((rows, tokens.shape[1]), BF16),
        ),
        in_specs=[anywhere] * 12,
        out_specs=(anywhere, anywhere),
        scratch_shapes=[
            vmem((q_rows, qk_width), BF16),
            vmem((1, 1), F32),
            vmem((1, v_width), F32),
            vmem(tokens.shape, BF16),
            vmem((pick_count, rows), jnp.int32),
            vmem((pick_count, rows), F32),
            vmem((n_z, 1, width // n_z), F32),
            vmem(gate_weight.shape, BF16),
            vmem(up_weight.shape, BF16),
            vmem(down_weight.shape, BF16),
            vmem((q_rows, v_width), BF16),
            vmem((rows, tokens.shape[1]), BF16),
            vmem((2 * q_rows, qk_width), BF16),
            vmem((n_ep, q_rows, qk_width), BF16),
            vmem((n_ep, q_rows, v_width), BF16),
            vmem((2 * q_rows, 2 * v_width), F32),
            vmem((2 * q_rows, 128), F32),
            vmem((2, rows, slots), BF16),
            vmem((slots, tokens.shape[1]), BF16),
            vmem((n_tp, slots, tokens.shape[1]), BF16),
            vmem((2, 2, 2, part, ff), F32),
            vmem((2, slots // 2, 128), F32),
            vmem((4, part, ff), BF16),
            vmem((2, n_z, 4, part, 128), BF16),
            vmem((n_z, 4, part, 128), BF16),
            vmem((4 * n_z, part, 128), BF16),
            vmem((4 * n_z, part, 128), BF16),
            vmem((slots, 128), BF16),
            vmem((slots, 128), BF16),
            dma((12,)),
            dma((2,)),
            dma((2,)),
            dma((len(STAGES) - 1,)),
            dma((1,)),
            dma((SIDE,)),
            dma((1,)),
            dma((4 * n_z,)),
            dma((1,)),
            dma((2 * n_z,)),
            dma((1,)),
            dma((2 * n_z,)),
            dma((1,)),
            dma((4 * n_z,)),
            dma((2,)),
        ],
        compiler_params=pltpu.CompilerParams(
            collective_id=0, has_side_effects=True, vmem_limit_bytes=60 * 1024 * 1024
        ),
    )(
        queries.reshape(q_rows, qk_width),
        keys.reshape(q_rows, qk_width),
        values.reshape(q_rows, v_width),
        mix_weight.reshape(1, 1),
        sub_gain.reshape(1, v_width),
        tokens,
        routes.T,
        route_weights.T,
        expert_gain.reshape(n_z, 1, width // n_z),
        gate_weight,
        up_weight,
        down_weight,
    )
    whole = pl.BlockSpec(memory_space=vmem)
    attn_out, moe_out = pl.pallas_call(
        hand_on,
        name="hand_on",
        out_shape=(
            jax.ShapeDtypeStruct(attn_out.shape, BF16),
            jax.ShapeDtypeStruct(moe_out.shape, BF16),
        ),
        in_specs=[whole] * 2,
        out_specs=(whole, whole),
    )(attn_out, moe_out)
    return attn_out.reshape(q_rows, 1, v_width), moe_out


def solution(mesh):
    return jax.shard_map(
        shards,
        mesh=mesh,
        in_specs=(
            P("ep", "tp", None),
            P("ep", "tp", None),
            P("ep", "tp", None),
            P("tp"),
            P(),
            P("ep", "tp"),
            P("ep", None),
            P("ep", None),
            P(),
            P("ep", None, "tp"),
            P("ep", None, "tp"),
            P("ep", "tp", None),
        ),
        out_specs=(P("ep", "tp", None), P("ep", "tp")),
        check_vma=False,
    )
```

```python
import functools
import math

import jax
import jax.numpy as jnp
from jax import lax
from jax.experimental import pallas as pl
from jax.experimental.pallas import tpu as pltpu
from jax.sharding import PartitionSpec as P

MESH = pl.DeviceIdType.MESH
NEG_FILL = -1e30
SUB_EPS = 1e-05
NORM_EPS = 1e-06
CLAMP_LIMIT = 7.0
GLU_ALPHA = 1.702
OUT_SCALE = 0.8
F32 = jnp.float32
BF16 = jnp.bfloat16


def nt_dot(a, b):
    return lax.dot_general(a, b, (((1,), (1,)), ((), ())), preferred_element_type=F32)


def nn_dot(a, b):
    return jnp.dot(a, b, preferred_element_type=F32)


STAGES = (
    ((), (((0, 0), "x+"), ((0, 0), "x-"), ((0, 0), "y+"), ((0, 0), "y-"))),
    (
        ((0, -1), (0, 1), (-1, 0), (1, 0)),
        (
            ((0, -1), "x+"),
            ((0, -1), "y+"),
            ((0, -1), "y-"),
            ((0, 1), "y+"),
            ((0, 1), "y-"),
            ((-1, 0), "y+"),
        ),
    ),
    (
        ((0, 2), (-1, -1), (1, -1), (-1, 1), (1, 1), (2, 0)),
        (((0, 2), "y+"), ((0, 2), "y-"), ((-1, -1), "y+"), ((1, 1), "y-")),
    ),
    (((-1, 2), (1, 2), (2, -1), (2, 1)), (((1, 2), "y-"),)),
    (((2, 2),), ()),
)
STEP = {"x+": (0, 1), "x-": (0, -1), "y+": (1, 0), "y-": (-1, 0)}
MIRROR = {"x+": "y-", "x-": "y+", "y+": "x-", "y-": "x+"}
SIDE = 4
ROW_ORDER = (0, 1, -1, 2)
FAR_FIRST = tuple(sorted(((a, b) for a in range(4) for b in range(4)), key=lambda p: -min(p[0], 4 - p[0]) - min(p[1], 4 - p[1])))[:-1]


def kernel(
    cfg,
    q_hbm,
    k_hbm,
    v_hbm,
    mix_hbm,
    sub_gain_hbm,
    tokens_hbm,
    routes_hbm,
    pick_weight_hbm,
    gain_hbm,
    gate_hbm,
    up_hbm,
    down_hbm,
    attn_hbm,
    moe_hbm,
    q_ref,
    mix_ref,
    sub_gain_ref,
    tokens_ref,
    routes_ref,
    pick_weight_ref,
    gain_ref,
    gate_w,
    up_w,
    down_w,
    attn_ref,
    moe_ref,
    qz,
    kbuf,
    vbuf,
    acc,
    row_max,
    picks,
    outgoing,
    gathered,
    pre,
    squares,
    hidden,
    ybuf,
    prec,
    rsend,
    rrecv,
    back_send,
    back,
    in_sem,
    out_sem,
    kv_send,
    kv_recv,
    d_send,
    d_recv,
    g_send,
    g_recv,
    p_send,
    p_recv,
    y_send,
    y_recv,
    r_send,
    r_recv,
    b_sem,
):
    n_ep, n_tp, cap, rows = cfg["n_ep"], cfg["n_tp"], cfg["cap"], cfg["rows"]
    n_z = n_tp // 2
    far = n_z // 2
    block = 2 * cap
    slots = n_ep * block
    half = slots // 2
    sources_half = n_ep // 2
    part = half // 2
    ep = lax.axis_index("ep")
    tp = lax.axis_index("tp")
    z, c = lax.div(tp, 2), lax.rem(tp, 2)
    py, px = lax.div(ep, SIDE), lax.rem(ep, SIDE)
    partner = tp + 1 - 2 * c

    def ring(at, shift):
        return lax.rem(at + shift + 2 * n_z, n_z)

    def remote(src, dst, send_sem, recv_sem, to_ep, to_tp):
        return pltpu.make_async_remote_copy(
            src_ref=src,
            dst_ref=dst,
            send_sem=send_sem,
            recv_sem=recv_sem,
            device_id=(to_ep, to_tp),
            device_id_type=MESH,
        )

    barrier = pltpu.get_barrier_semaphore()
    def across(dy, dx):
        return lax.rem(py + dy + SIDE, SIDE) * SIDE + lax.rem(px + dx + SIDE, SIDE)

    for dy, dx in FAR_FIRST:
        pl.semaphore_signal(barrier, inc=1, device_id=(across(dy, dx), tp), device_id_type=MESH)
    for to in (2 * ring(z, 1) + c, 2 * ring(z, -1) + c, partner):
        pl.semaphore_signal(barrier, inc=1, device_id=(ep, to), device_id_type=MESH)

    loads = [
        pltpu.make_async_copy(src, dst, in_sem.at[i])
        for i, (src, dst) in enumerate(
            (
                (routes_hbm, routes_ref),
                (tokens_hbm, tokens_ref),
                (q_hbm, q_ref),
                (k_hbm, kbuf.at[0]),
                (v_hbm, vbuf.at[0]),
                (gain_hbm, gain_ref),
                (gate_hbm, gate_w),
                (up_hbm, up_w),
                (down_hbm, down_w),
                (mix_hbm, mix_ref),
                (sub_gain_hbm, sub_gain_ref),
                (pick_weight_hbm, pick_weight_ref),
            )
        )
    ]
    for copy in loads:
        copy.start()

    for copy in loads[:2]:
        copy.wait()
    pairs = 2 * rows
    experts = 2 * n_ep
    routes = jnp.concatenate([routes_ref[0:1, :], routes_ref[1:2, :]], axis=1)
    member = (
        lax.broadcasted_iota(jnp.int32, (experts, pairs), 0)
        == jnp.broadcast_to(routes, (experts, pairs))
    ).astype(F32)

    def order(dim):
        at = lax.broadcasted_iota(jnp.int32, (pairs, pairs), dim)
        return jnp.where(at < rows, 2 * at, 2 * (at - rows) + 1)

    earlier = (order(0) < order(1)).astype(F32).astype(BF16)
    rank = nn_dot(member.astype(BF16), earlier)
    first_slot = lax.broadcasted_iota(jnp.int32, (experts, pairs), 0).astype(F32) * float(cap)
    target = jnp.sum(member * (rank + first_slot), axis=0, keepdims=True)
    slot_at = lax.broadcasted_iota(jnp.int32, (slots, rows), 0).astype(F32)
    pick_0 = (slot_at == jnp.broadcast_to(target[:, :rows], (slots, rows))).astype(F32)
    pick_1 = (slot_at == jnp.broadcast_to(target[:, rows:], (slots, rows))).astype(F32)
    out_rows = nn_dot((pick_0 + pick_1).astype(BF16), tokens_ref[...]).astype(BF16)
    outgoing[...] = out_rows
    mine = pl.ds(pl.multiple_of(ep * block, block), block)
    own = pl.ds(pl.multiple_of(px * block, block), block)
    gathered[tp, own, :] = outgoing[mine, :]

    loads[2].wait()
    q_all = q_ref[...]
    q_rows = q_all.shape[0]
    lane = lax.broadcasted_iota(jnp.int32, q_all.shape, 1)
    zero = jnp.zeros_like(q_all)
    qz[:q_rows] = jnp.where(lane < q_all.shape[1] // 2, q_all, zero)
    qz[q_rows:] = jnp.where(lane >= q_all.shape[1] // 2, q_all, zero)

    pl.semaphore_wait(barrier, n_ep - 1 + 3)

    for group, dy in enumerate(ROW_ORDER):
        for dx in range(SIDE):
            if dy == 0 and dx == 0:
                continue
            to = across(-dy, dx)
            at = pl.multiple_of((group * SIDE + px) * block, block)
            remote(
                outgoing.at[pl.ds(pl.multiple_of(to * block, block), block)],
                gathered.at[tp, pl.ds(at, block)],
                d_send.at[0],
                d_recv.at[group],
                to,
                tp,
            ).start()
    others = (n_ep - 1) * block

    exponent = (q_ref.shape[1] // 2) ** (-0.5) * math.log2(math.e)
    width = vbuf.shape[2]
    tile = min(256, q_rows)

    def scores_at(r, keys, first):
        scores = nt_dot(qz[pl.ds(r, tile), :], keys)
        if first:
            seen = lax.broadcasted_iota(jnp.int32, scores.shape, 1) <= (
                lax.broadcasted_iota(jnp.int32, scores.shape, 0) + r % q_rows
            )
            scores = jnp.where(seen, scores, NEG_FILL)
        return scores

    def attend(held, maps=(0, 1), first=False):
        keys = jnp.concatenate([kbuf[s] for s in held], axis=0)
        values = jnp.concatenate([vbuf[s] for s in held], axis=0)
        both = jnp.concatenate([values, jnp.ones_like(values)], axis=1)
        at = [m * q_rows + r for m in maps for r in range(0, q_rows, tile)]
        scores = [scores_at(r, keys, first) for r in at]
        tops = [jnp.max(s, axis=1, keepdims=True) for s in scores]
        if first:
            tops = [jnp.broadcast_to(t, (tile, 128)) for t in tops]
        else:
            olds = [row_max[pl.ds(r, tile), :] for r in at]
            tops = [jnp.maximum(o, t) for o, t in zip(olds, tops)]
        weights = [
            jnp.exp2((s - jnp.concatenate([t] * (s.shape[1] // 128), axis=1)) * exponent).astype(
                BF16
            )
            for s, t in zip(scores, tops)
        ]
        for i, r in enumerate(at):
            where = pl.ds(r, tile)
            added = nn_dot(weights[i], both)
            if first:
                acc[where, :] = added
            else:
                shrink = jnp.exp2((olds[i] - tops[i]) * exponent)
                acc[where, :] = acc[where, :] * jnp.concatenate([shrink, shrink], axis=1) + added
            row_max[where, :] = tops[i]

    def held_at(a, b):
        return (a % SIDE) * SIDE + b % SIDE

    def spread(stage):
        waits, sends = STAGES[stage]
        if waits:
            all_of = kbuf.at[pl.ds(0, 2 * len(waits))]
            remote(all_of, all_of, kv_send.at[0], kv_recv.at[stage - 1], ep, partner).wait_recv()
        for (a, b), way in sends:
            for n, buf in enumerate((kbuf, vbuf)):
                if n == 1:
                    a, b, way = -b, -a, MIRROR[way]
                dy, dx = STEP[way]
                to = across(dy, dx)
                at = held_at(a - dy, b - dx)
                remote(
                    buf.at[held_at(a, b)], buf.at[at], kv_send.at[n], kv_recv.at[stage], to, tp
                ).start()

    for copy in loads[3:5]:
        copy.wait()
    attend((0,), first=True)

    column = jnp.broadcast_to(target, (128, pairs)).T
    slot_on = lax.broadcasted_iota(jnp.int32, (rows, 128), 1).astype(F32)
    for n in range(2):
        at_row = column[n * rows : (n + 1) * rows]
        for s0 in range(0, slots, 128):
            picks[n, :, s0 : s0 + 128] = (slot_on + float(s0) == at_row).astype(F32).astype(BF16)
    cut = half // 2

    def source_of(way, hop):
        return ring(z, -hop) if way == 0 else ring(z, hop)

    def gather_copy(way, hop, sub):
        to = ring(z, 1) if way == 0 else ring(z, -1)
        piece = gathered.at[2 * source_of(way, hop) + c, pl.ds(sub * cut, cut)]
        at = (way * far + hop) * 4 + sub
        return remote(piece, piece, g_send.at[0], g_recv.at[at], ep, 2 * to + c)

    def gather_wait(way, hop, sub):
        piece = gathered.at[2 * source_of(way, hop) + c, pl.ds(sub * cut, cut)]
        at = (way * far + hop - 1) * 4 + sub
        remote(piece, piece, g_send.at[0], g_recv.at[at], ep, partner).wait_recv()

    def subs_of(way, hop):
        return range(4) if hop < far - 1 else range(way, 4, 2)

    def sub_at(way, step):
        return step if way == 0 else step // 2 * 2 + 1 - step % 2

    def shard(way, hop):
        return 0 if hop == 0 else (2 * hop - 1 + way if hop < far else n_z - 1)

    def partner_copy(way, hop, h, core):
        piece = gathered.at[2 * source_of(way, hop) + core, pl.ds(h * half, half)]
        return remote(
            piece, piece, p_send.at[0], p_recv.at[shard(way, hop) * 2 + h], ep, partner
        )

    for sub in range(4):
        group = gathered.at[tp, pl.ds(0, (SIDE - 1 if sub == 0 else SIDE) * block)]
        remote(group, group, d_send.at[0], d_recv.at[sub], ep, partner).wait_recv()
        if sub % 2 == 0:
            gather_copy(0, 0, sub).start()
        else:
            gather_copy(1, 0, sub).start()
            gather_copy(0, 0, sub).start()
            gather_copy(1, 0, sub - 1).start()
            partner_copy(0, 0, sub // 2, c).start()

    def by_expert(value):
        w = value.shape[1]
        cut_up = value.reshape(sources_half, 2, cap, w)
        return [cut_up[:, e].reshape(part, w) for e in range(2)]

    def expert_in(way, hop, h):
        source = source_of(way, hop)
        partner_copy(way, hop, h, 1 - c).wait_recv()
        at = pl.ds(h * half, half)
        x = jnp.concatenate(
            [gathered[2 * source, at, :], gathered[2 * source + 1, at, :]], axis=1
        ).astype(F32)
        square = jnp.broadcast_to(jnp.sum(x * x, axis=1, keepdims=True), (half, 128))
        squares[h] = square if hop == 0 else squares[h] + square
        depth = x.shape[1]
        deep = pl.ds(pl.multiple_of(source * depth, depth), depth)
        for e, rows_e in enumerate(by_expert(x * gain_ref[source])):
            rows_e = rows_e.astype(BF16)
            for n, w in enumerate((gate_w, up_w)):
                product = nn_dot(rows_e, w[e, deep, :])
                pre[h, e, n] = product if hop == 0 else pre[h, e, n] + product

    spread(0)
    for copy in loads[5:]:
        copy.wait()
    for h in range(2):
        expert_in(0, 0, h)

    y_1, y_2, y_3 = py >= 1, py >= 2, py >= 3
    x_1, x_2, x_3 = px >= 1, px >= 2, px >= 3

    def pieces(*cases):
        def work(m):
            taken = None
            for cond, places in cases:
                now = cond if taken is None else jnp.logical_and(cond, jnp.logical_not(taken))

                @pl.when(now)
                def _(places=places):
                    attend([held_at(a, b) for a, b in places], (m,))

                taken = cond if taken is None else jnp.logical_or(taken, cond)

        return [functools.partial(work, 0), functools.partial(work, 1)]

    both_2 = jnp.logical_and(x_2, y_2)
    mid = [
        *pieces((y_1, ((-1, -1), (-1, 1)))),
        *pieces((y_3, ((1, -1), (1, 1)))),
        *pieces((both_2, ((0, 2), (2, 0))), (x_2, ((0, 2),)), (y_2, ((2, 0),))),
    ]

    def rest():
        pass

    fillers = [
        *pieces((y_3, ((-1, 0), (1, 0))), (y_1, ((-1, 0),))),
        *pieces((x_3, ((0, -1), (0, 1))), (x_1, ((0, -1),))),
        lambda: spread(2),
        rest,
        *mid[:3],
        rest,
        *mid[3:],
        lambda: spread(3),
        *pieces((y_3, ((-1, 2), (1, 2))), (y_1, ((-1, 2),))),
        *pieces((y_2, ((2, -1), (2, 1)))),
    ]
    last_fillers = [lambda: spread(4), *pieces((y_2, ((2, 2),)))]

    def fill(count=1):
        for _ in range(count):
            if fillers:
                fillers.pop(0)()

    def activate(h):
        factor = lax.rsqrt(squares[h] / float(cfg["width"]) + NORM_EPS)
        for e, f in enumerate(by_expert(factor)):
            f = jnp.concatenate([f, f], axis=1)
            gate = jnp.minimum(pre[h, e, 0] * f, CLAMP_LIMIT)
            up = jnp.clip(pre[h, e, 1] * f, -CLAMP_LIMIT, CLAMP_LIMIT)
            hidden[2 * h + e] = ((up + 1.0) * gate * jax.nn.sigmoid(GLU_ALPHA * gate)).astype(
                BF16
            )

    for hop in range(1, far):
        for step in range(4):
            if (hop, step) == (2, 2):
                spread(1)
            for way in range(2):
                sub = sub_at(way, step)
                gather_wait(way, hop, sub)
                if sub in subs_of(way, hop):
                    gather_copy(way, hop, sub).start()
            if step % 2 == 1:
                for way in range(2):
                    partner_copy(way, hop, step // 2, c).start()
            if step == 0 and hop > 1:
                for way in range(2):
                    expert_in(way, hop - 1, 1)
            if step == 2:
                for way in range(2):
                    expert_in(way, hop, 0)
            if (hop, step) in ((2, 2), (2, 3), (3, 1), (3, 3)):
                fill()

    def gather_last(h):
        for way in range(2):
            gather_wait(way, far, 2 * h + way)
        partner_copy(0, far, h, c).start()

    goals = [ring(z, far)]
    for hop in range(1, far):
        goals += [ring(z, far - hop), ring(z, hop - far)]
    goals += [z]

    def goal_of(way, hop):
        return 0 if hop == 0 else 2 * hop - 1 + way

    def down(g, h):
        wide = pl.ds(pl.multiple_of(goals[g] * 256, 256), 256)
        for e in range(2):
            y = nn_dot(hidden[2 * h + e], down_w[e, :, wide]).astype(BF16)
            ybuf[0, g, 2 * h + e] = y[:, :128]
            ybuf[1, g, 2 * h + e] = y[:, 128:]
        y_copy(g, h).start()

    def y_copy(g, h):
        at = pl.ds(2 * h, 2)
        return remote(
            ybuf.at[1 - c, g, at],
            prec.at[g, at],
            y_send.at[0],
            y_recv.at[2 * g + h],
            ep,
            partner,
        )

    def sum_copy(way, hop, he):
        to = ring(z, 1) if way == 0 else ring(z, -1)
        at = (way * far + hop) * 4 + he
        return remote(
            rsend.at[at], rrecv.at[at], r_send.at[0], r_recv.at[at], ep, 2 * to + c
        )

    def own_sum(g, he):
        return ybuf[c, g, he].astype(F32) + prec[g, he].astype(F32)

    def arrived_sum(total, way, hop, he):
        if hop > 0 or he % 2 == way:
            sum_copy(way, hop, he).wait_recv()
            total = total + rrecv[(way * far + hop) * 4 + he].astype(F32)
        return total

    def pass_on(way, hop, he):
        total = own_sum(goal_of(way, hop), he)
        if hop > 0:
            total = arrived_sum(total, way, hop - 1, he)
        rsend[(way * far + hop) * 4 + he] = total.astype(BF16)
        sum_copy(way, hop, he).start()

    def begin(h):
        y_copy(0, h).wait_recv()
        for way in range(2):
            pass_on(way, 0, 2 * h + way)

    def fresh(h):
        for way in range(2):
            y_copy(goal_of(way, 1), h).wait_recv()
            pass_on(way, 1, 2 * h + 1 - way)

    def finish_expert(h):
        expert_in(0, far, h)
        activate(h)
        down(0, h)

    gather_last(0)
    for way in range(2):
        expert_in(way, far - 1, 1)
    finish_expert(0)
    for g in (1, 2):
        down(g, 0)
    gather_last(1)
    begin(0)
    finish_expert(1)
    fresh(0)
    for g in (1, 2):
        down(g, 1)
    begin(1)
    fresh(1)
    for g in (3, 4):
        for h in range(2):
            down(g, h)

    for hop in range(1, far):
        if hop > 1:
            for way in range(2):
                for h in range(2):
                    y_copy(goal_of(way, hop), h).wait_recv()
        for step in range(2 if hop == 1 else 0, 4):
            fill()
            for way in range(2):
                e = 1 - way if step < 2 else way
                pass_on(way, hop, step % 2 * 2 + e)
            if step == 2:
                for g in {1: (5, 6), 2: (7,), 3: ()}[hop]:
                    for h in range(2):
                        down(g, h)

    last = n_z - 1
    for h in range(2):
        y_copy(last, h).wait_recv()
    for h in range(2):
        totals = []
        for e in range(2):
            he = 2 * h + e
            if he == 0:
                fill(2)
            total = own_sum(last, he)
            for way in range(2):
                total = arrived_sum(total, way, far - 1, he)
            totals.append(total.reshape(sources_half, 1, cap, 128))
        back_send[h * half : (h + 1) * half] = (
            jnp.concatenate(totals, axis=1).reshape(half, 128).astype(BF16)
        )
        for p in reversed(range(h * sources_half, (h + 1) * sources_half)):

            @pl.when(px != p)
            def _(p=p):
                to = lax.rem(py + ROW_ORDER[p // SIDE] + SIDE, SIDE) * SIDE + p % SIDE
                remote(
                    back_send.at[pl.ds(p * block, block)],
                    back.at[mine],
                    b_sem.at[0],
                    b_sem.at[1],
                    to,
                    tp,
                ).start()

    back[mine, :] = back_send[own, :]
    fillers += last_fillers
    fill(len(fillers))

    mix = mix_ref[...]
    for r in range(0, q_rows, tile):
        one, two = pl.ds(r, tile), pl.ds(q_rows + r, tile)
        blend = acc[one, :width] / acc[one, width:] - mix * (acc[two, :width] / acc[two, width:])
        mean = jnp.mean(blend * blend, axis=1, keepdims=True)
        scaled = blend * lax.rsqrt(mean + SUB_EPS)
        attn_ref[one, :] = (scaled * sub_gain_ref[...] * OUT_SCALE).astype(BF16)
    attn_out = pltpu.make_async_copy(attn_ref, attn_hbm, out_sem.at[0])
    attn_out.start()

    sent = outgoing.at[pl.ds(0, others)]
    remote(sent, sent, d_send.at[0], d_recv.at[0], ep, partner).wait_send()
    for n, buf in enumerate((kbuf, vbuf)):
        whole = buf.at[pl.ds(0, n_ep - 1)]
        remote(whole, whole, kv_send.at[n], kv_recv.at[0], ep, partner).wait_send()
    whole = gathered.at[pl.ds(0, n_z - 1)]
    remote(whole, whole, g_send.at[0], g_recv.at[0], ep, partner).wait_send()
    whole = gathered.at[pl.ds(0, n_z)]
    remote(whole, whole, p_send.at[0], p_recv.at[0], ep, partner).wait_send()
    remote(ybuf.at[0], prec, y_send.at[0], y_recv.at[0], ep, partner).wait_send()
    sent = pl.ds(0, 4 * (n_z - 1))
    remote(rsend.at[sent], rrecv.at[sent], r_send.at[0], r_recv.at[0], ep, partner).wait_send()
    weight = jnp.concatenate(
        [pick_weight_ref[...], jnp.zeros((126, rows), F32)], axis=0
    ).T

    piece = back.at[pl.ds(0, others)]
    remote(piece, piece, b_sem.at[0], b_sem.at[1], ep, partner).wait()
    result = back[...]
    moe_ref[...] = (
        nn_dot(picks[0], result) * weight[:, 0:1] + nn_dot(picks[1], result) * weight[:, 1:2]
    ).astype(BF16)
    moe_out = pltpu.make_async_copy(moe_ref, moe_hbm, out_sem.at[1])
    moe_out.start()
    attn_out.wait()
    moe_out.wait()


def hand_on(attn_in, moe_in, attn_ref, moe_ref):
    attn_ref[...] = attn_in[...]
    moe_ref[...] = moe_in[...]


def shards(
    queries,
    keys,
    values,
    mix_weight,
    sub_gain,
    tokens,
    routes,
    route_weights,
    expert_gain,
    gate_weight,
    up_weight,
    down_weight,
):
    n_ep, n_tp = lax.axis_size("ep"), lax.axis_size("tp")
    n_z = n_tp // 2
    rows, pick_count = routes.shape
    experts = n_ep * gate_weight.shape[0]
    cap = 3 * rows * pick_count // (2 * experts)
    slots = experts * cap
    part = slots // 4
    q_rows, _, qk_width = queries.shape
    v_width = values.shape[2]
    width = expert_gain.shape[0]
    ff = gate_weight.shape[2]
    cfg = dict(n_ep=n_ep, n_tp=n_tp, cap=cap, rows=rows, width=width)
    dma = pltpu.SemaphoreType.DMA
    vmem = pltpu.VMEM
    anywhere = pl.BlockSpec(memory_space=pl.ANY)
    attn_out, moe_out = pl.pallas_call(
        functools.partial(kernel, cfg),
        name="layer",
        out_shape=(
            jax.ShapeDtypeStruct((q_rows, v_width), BF16),
            jax.ShapeDtypeStruct((rows, tokens.shape[1]), BF16),
        ),
        in_specs=[anywhere] * 12,
        out_specs=(anywhere, anywhere),
        scratch_shapes=[
            vmem((q_rows, qk_width), BF16),
            vmem((1, 1), F32),
            vmem((1, v_width), F32),
            vmem(tokens.shape, BF16),
            vmem((pick_count, rows), jnp.int32),
            vmem((pick_count, rows), F32),
            vmem((n_z, 1, width // n_z), F32),
            vmem(gate_weight.shape, BF16),
            vmem(up_weight.shape, BF16),
            vmem(down_weight.shape, BF16),
            vmem((q_rows, v_width), BF16),
            vmem((rows, tokens.shape[1]), BF16),
            vmem((2 * q_rows, qk_width), BF16),
            vmem((n_ep, q_rows, qk_width), BF16),
            vmem((n_ep, q_rows, v_width), BF16),
            vmem((2 * q_rows, 2 * v_width), F32),
            vmem((2 * q_rows, 128), F32),
            vmem((2, rows, slots), BF16),
            vmem((slots, tokens.shape[1]), BF16),
            vmem((n_tp, slots, tokens.shape[1]), BF16),
            vmem((2, 2, 2, part, ff), F32),
            vmem((2, slots // 2, 128), F32),
            vmem((4, part, ff), BF16),
            vmem((2, n_z, 4, part, 128), BF16),
            vmem((n_z, 4, part, 128), BF16),
            vmem((4 * n_z, part, 128), BF16),
            vmem((4 * n_z, part, 128), BF16),
            vmem((slots, 128), BF16),
            vmem((slots, 128), BF16),
            dma((12,)),
            dma((2,)),
            dma((2,)),
            dma((len(STAGES) - 1,)),
            dma((1,)),
            dma((SIDE,)),
            dma((1,)),
            dma((4 * n_z,)),
            dma((1,)),
            dma((2 * n_z,)),
            dma((1,)),
            dma((2 * n_z,)),
            dma((1,)),
            dma((4 * n_z,)),
            dma((2,)),
        ],
        compiler_params=pltpu.CompilerParams(
            collective_id=0, has_side_effects=True, vmem_limit_bytes=60 * 1024 * 1024
        ),
    )(
        queries.reshape(q_rows, qk_width),
        keys.reshape(q_rows, qk_width),
        values.reshape(q_rows, v_width),
        mix_weight.reshape(1, 1),
        sub_gain.reshape(1, v_width),
        tokens,
        routes.T,
        route_weights.T,
        expert_gain.reshape(n_z, 1, width // n_z),
        gate_weight,
        up_weight,
        down_weight,
    )
    whole = pl.BlockSpec(memory_space=vmem)
    attn_out, moe_out = pl.pallas_call(
        hand_on,
        name="hand_on",
        out_shape=(
            jax.ShapeDtypeStruct(attn_out.shape, BF16),
            jax.ShapeDtypeStruct(moe_out.shape, BF16),
        ),
        in_specs=[whole] * 2,
        out_specs=(whole, whole),
    )(attn_out, moe_out)
    return attn_out.reshape(q_rows, 1, v_width), moe_out


def solution(mesh):
    return jax.shard_map(
        shards,
        mesh=mesh,
        in_specs=(
            P("ep", "tp", None),
            P("ep", "tp", None),
            P("ep", "tp", None),
            P("tp"),
            P(),
            P("ep", "tp"),
            P("ep", None),
            P("ep", None),
            P(),
            P("ep", None, "tp"),
            P("ep", None, "tp"),
            P("ep", "tp", None),
        ),
        out_specs=(P("ep", "tp", None), P("ep", "tp")),
        check_vma=False,
    )
```

```python
import functools
import math

import jax
import jax.numpy as jnp
from jax import lax
from jax.experimental import pallas as pl
from jax.experimental.pallas import tpu as pltpu
from jax.sharding import PartitionSpec as P

MESH = pl.DeviceIdType.MESH
NEG_FILL = -1e30
SUB_EPS = 1e-05
NORM_EPS = 1e-06
CLAMP_LIMIT = 7.0
GLU_ALPHA = 1.702
OUT_SCALE = 0.8
F32 = jnp.float32
BF16 = jnp.bfloat16


def nt_dot(a, b):
    return lax.dot_general(a, b, (((1,), (1,)), ((), ())), preferred_element_type=F32)


def nn_dot(a, b):
    return jnp.dot(a, b, preferred_element_type=F32)


STAGES = (
    ((), (((0, 0), "x+"), ((0, 0), "x-"), ((0, 0), "y+"), ((0, 0), "y-"))),
    (
        ((0, -1), (0, 1), (-1, 0), (1, 0)),
        (
            ((0, -1), "x+"),
            ((0, -1), "y+"),
            ((0, -1), "y-"),
            ((0, 1), "y+"),
            ((0, 1), "y-"),
            ((-1, 0), "y+"),
        ),
    ),
    (
        ((0, 2), (-1, -1), (1, -1), (-1, 1), (1, 1), (2, 0)),
        (((0, 2), "y+"), ((0, 2), "y-"), ((-1, -1), "y+"), ((1, 1), "y-")),
    ),
    (((-1, 2), (1, 2), (2, -1), (2, 1)), (((1, 2), "y-"),)),
    (((2, 2),), ()),
)
STEP = {"x+": (0, 1), "x-": (0, -1), "y+": (1, 0), "y-": (-1, 0)}
MIRROR = {"x+": "y-", "x-": "y+", "y+": "x-", "y-": "x+"}
SIDE = 4
ROW_ORDER = (0, 1, -1, 2)
FAR_FIRST = tuple(sorted(((a, b) for a in range(4) for b in range(4)), key=lambda p: -min(p[0], 4 - p[0]) - min(p[1], 4 - p[1])))[:-1]


def kernel(
    cfg,
    q_hbm,
    k_hbm,
    v_hbm,
    mix_hbm,
    sub_gain_hbm,
    tokens_hbm,
    routes_hbm,
    pick_weight_hbm,
    gain_hbm,
    gate_hbm,
    up_hbm,
    down_hbm,
    attn_ref,
    moe_ref,
    q_ref,
    mix_ref,
    sub_gain_ref,
    tokens_ref,
    routes_ref,
    pick_weight_ref,
    gain_ref,
    gate_w,
    up_w,
    down_w,
    qz,
    kbuf,
    vbuf,
    acc,
    row_max,
    picks,
    outgoing,
    gathered,
    pre,
    squares,
    hidden,
    ybuf,
    prec,
    rsend,
    rrecv,
    back_send,
    back,
    in_sem,
    kv_send,
    kv_recv,
    d_send,
    d_recv,
    g_send,
    g_recv,
    p_send,
    p_recv,
    y_send,
    y_recv,
    r_send,
    r_recv,
    b_sem,
):
    n_ep, n_tp, cap, rows = cfg["n_ep"], cfg["n_tp"], cfg["cap"], cfg["rows"]
    n_z = n_tp // 2
    far = n_z // 2
    block = 2 * cap
    slots = n_ep * block
    half = slots // 2
    sources_half = n_ep // 2
    part = half // 2
    ep = lax.axis_index("ep")
    tp = lax.axis_index("tp")
    z, c = lax.div(tp, 2), lax.rem(tp, 2)
    py, px = lax.div(ep, SIDE), lax.rem(ep, SIDE)
    partner = tp + 1 - 2 * c

    def ring(at, shift):
        return lax.rem(at + shift + 2 * n_z, n_z)

    def remote(src, dst, send_sem, recv_sem, to_ep, to_tp):
        return pltpu.make_async_remote_copy(
            src_ref=src,
            dst_ref=dst,
            send_sem=send_sem,
            recv_sem=recv_sem,
            device_id=(to_ep, to_tp),
            device_id_type=MESH,
        )

    barrier = pltpu.get_barrier_semaphore()
    def across(dy, dx):
        return lax.rem(py + dy + SIDE, SIDE) * SIDE + lax.rem(px + dx + SIDE, SIDE)

    for dy, dx in FAR_FIRST:
        pl.semaphore_signal(barrier, inc=1, device_id=(across(dy, dx), tp), device_id_type=MESH)
    for to in (2 * ring(z, 1) + c, 2 * ring(z, -1) + c, partner):
        pl.semaphore_signal(barrier, inc=1, device_id=(ep, to), device_id_type=MESH)

    loads = [
        pltpu.make_async_copy(src, dst, in_sem.at[i])
        for i, (src, dst) in enumerate(
            (
                (routes_hbm, routes_ref),
                (tokens_hbm, tokens_ref),
                (q_hbm, q_ref),
                (k_hbm, kbuf.at[0]),
                (v_hbm, vbuf.at[0]),
                (gain_hbm, gain_ref),
                (gate_hbm, gate_w),
                (up_hbm, up_w),
                (down_hbm, down_w),
                (mix_hbm, mix_ref),
                (sub_gain_hbm, sub_gain_ref),
                (pick_weight_hbm, pick_weight_ref),
            )
        )
    ]
    for copy in loads:
        copy.start()

    for copy in loads[:2]:
        copy.wait()
    pairs = 2 * rows
    experts = 2 * n_ep
    routes = jnp.concatenate([routes_ref[0:1, :], routes_ref[1:2, :]], axis=1)
    member = (
        lax.broadcasted_iota(jnp.int32, (experts, pairs), 0)
        == jnp.broadcast_to(routes, (experts, pairs))
    ).astype(F32)

    def order(dim):
        at = lax.broadcasted_iota(jnp.int32, (pairs, pairs), dim)
        return jnp.where(at < rows, 2 * at, 2 * (at - rows) + 1)

    earlier = (order(0) < order(1)).astype(F32).astype(BF16)
    rank = nn_dot(member.astype(BF16), earlier)
    first_slot = lax.broadcasted_iota(jnp.int32, (experts, pairs), 0).astype(F32) * float(cap)
    target = jnp.sum(member * (rank + first_slot), axis=0, keepdims=True)
    slot_at = lax.broadcasted_iota(jnp.int32, (slots, rows), 0).astype(F32)
    pick_0 = (slot_at == jnp.broadcast_to(target[:, :rows], (slots, rows))).astype(F32)
    pick_1 = (slot_at == jnp.broadcast_to(target[:, rows:], (slots, rows))).astype(F32)
    out_rows = nn_dot((pick_0 + pick_1).astype(BF16), tokens_ref[...]).astype(BF16)
    outgoing[...] = out_rows
    mine = pl.ds(pl.multiple_of(ep * block, block), block)
    own = pl.ds(pl.multiple_of(px * block, block), block)
    gathered[tp, own, :] = outgoing[mine, :]

    loads[2].wait()
    q_all = q_ref[...]
    q_rows = q_all.shape[0]
    lane = lax.broadcasted_iota(jnp.int32, q_all.shape, 1)
    zero = jnp.zeros_like(q_all)
    qz[:q_rows] = jnp.where(lane < q_all.shape[1] // 2, q_all, zero)
    qz[q_rows:] = jnp.where(lane >= q_all.shape[1] // 2, q_all, zero)

    pl.semaphore_wait(barrier, n_ep - 1 + 3)

    for group, dy in enumerate(ROW_ORDER):
        for dx in range(SIDE):
            if dy == 0 and dx == 0:
                continue
            to = across(-dy, dx)
            at = pl.multiple_of((group * SIDE + px) * block, block)
            remote(
                outgoing.at[pl.ds(pl.multiple_of(to * block, block), block)],
                gathered.at[tp, pl.ds(at, block)],
                d_send.at[0],
                d_recv.at[group],
                to,
                tp,
            ).start()
    others = (n_ep - 1) * block

    exponent = (q_ref.shape[1] // 2) ** (-0.5) * math.log2(math.e)
    width = vbuf.shape[2]
    tile = min(256, q_rows)

    def scores_at(r, keys, first):
        scores = nt_dot(qz[pl.ds(r, tile), :], keys)
        if first:
            seen = lax.broadcasted_iota(jnp.int32, scores.shape, 1) <= (
                lax.broadcasted_iota(jnp.int32, scores.shape, 0) + r % q_rows
            )
            scores = jnp.where(seen, scores, NEG_FILL)
        return scores

    def attend(held, maps=(0, 1), first=False):
        keys = jnp.concatenate([kbuf[s] for s in held], axis=0)
        values = jnp.concatenate([vbuf[s] for s in held], axis=0)
        both = jnp.concatenate([values, jnp.ones_like(values)], axis=1)
        at = [m * q_rows + r for m in maps for r in range(0, q_rows, tile)]
        scores = [scores_at(r, keys, first) for r in at]
        tops = [jnp.max(s, axis=1, keepdims=True) for s in scores]
        if first:
            tops = [jnp.broadcast_to(t, (tile, 128)) for t in tops]
        else:
            olds = [row_max[pl.ds(r, tile), :] for r in at]
            tops = [jnp.maximum(o, t) for o, t in zip(olds, tops)]
        weights = [
            jnp.exp2((s - jnp.concatenate([t] * (s.shape[1] // 128), axis=1)) * exponent).astype(
                BF16
            )
            for s, t in zip(scores, tops)
        ]
        for i, r in enumerate(at):
            where = pl.ds(r, tile)
            added = nn_dot(weights[i], both)
            if first:
                acc[where, :] = added
            else:
                shrink = jnp.exp2((olds[i] - tops[i]) * exponent)
                acc[where, :] = acc[where, :] * jnp.concatenate([shrink, shrink], axis=1) + added
            row_max[where, :] = tops[i]

    def held_at(a, b):
        return (a % SIDE) * SIDE + b % SIDE

    def spread(stage):
        waits, sends = STAGES[stage]
        if waits:
            all_of = kbuf.at[pl.ds(0, 2 * len(waits))]
            remote(all_of, all_of, kv_send.at[0], kv_recv.at[stage - 1], ep, partner).wait_recv()
        for (a, b), way in sends:
            for n, buf in enumerate((kbuf, vbuf)):
                if n == 1:
                    a, b, way = -b, -a, MIRROR[way]
                dy, dx = STEP[way]
                to = across(dy, dx)
                at = held_at(a - dy, b - dx)
                remote(
                    buf.at[held_at(a, b)], buf.at[at], kv_send.at[n], kv_recv.at[stage], to, tp
                ).start()

    for copy in loads[3:5]:
        copy.wait()
    attend((0,), first=True)

    column = jnp.broadcast_to(target, (128, pairs)).T
    slot_on = lax.broadcasted_iota(jnp.int32, (rows, 128), 1).astype(F32)
    for n in range(2):
        at_row = column[n * rows : (n + 1) * rows]
        for s0 in range(0, slots, 128):
            picks[n, :, s0 : s0 + 128] = (slot_on + float(s0) == at_row).astype(F32).astype(BF16)
    cut = half // 2

    def source_of(way, hop):
        return ring(z, -hop) if way == 0 else ring(z, hop)

    def gather_copy(way, hop, sub):
        to = ring(z, 1) if way == 0 else ring(z, -1)
        piece = gathered.at[2 * source_of(way, hop) + c, pl.ds(sub * cut, cut)]
        at = (way * far + hop) * 4 + sub
        return remote(piece, piece, g_send.at[0], g_recv.at[at], ep, 2 * to + c)

    def gather_wait(way, hop, sub):
        piece = gathered.at[2 * source_of(way, hop) + c, pl.ds(sub * cut, cut)]
        at = (way * far + hop - 1) * 4 + sub
        remote(piece, piece, g_send.at[0], g_recv.at[at], ep, partner).wait_recv()

    def subs_of(way, hop):
        return range(4) if hop < far - 1 else range(way, 4, 2)

    def sub_at(way, step):
        return step if way == 0 else step // 2 * 2 + 1 - step % 2

    def shard(way, hop):
        return 0 if hop == 0 else (2 * hop - 1 + way if hop < far else n_z - 1)

    def partner_copy(way, hop, h, core):
        piece = gathered.at[2 * source_of(way, hop) + core, pl.ds(h * half, half)]
        return remote(
            piece, piece, p_send.at[0], p_recv.at[shard(way, hop) * 2 + h], ep, partner
        )

    for sub in range(4):
        group = gathered.at[tp, pl.ds(0, (SIDE - 1 if sub == 0 else SIDE) * block)]
        remote(group, group, d_send.at[0], d_recv.at[sub], ep, partner).wait_recv()
        if sub % 2 == 0:
            gather_copy(0, 0, sub).start()
        else:
            gather_copy(1, 0, sub).start()
            gather_copy(0, 0, sub).start()
            gather_copy(1, 0, sub - 1).start()
            partner_copy(0, 0, sub // 2, c).start()

    def by_expert(value):
        w = value.shape[1]
        cut_up = value.reshape(sources_half, 2, cap, w)
        return [cut_up[:, e].reshape(part, w) for e in range(2)]

    def expert_in(way, hop, h):
        source = source_of(way, hop)
        partner_copy(way, hop, h, 1 - c).wait_recv()
        at = pl.ds(h * half, half)
        x = jnp.concatenate(
            [gathered[2 * source, at, :], gathered[2 * source + 1, at, :]], axis=1
        ).astype(F32)
        square = jnp.broadcast_to(jnp.sum(x * x, axis=1, keepdims=True), (half, 128))
        squares[h] = square if hop == 0 else squares[h] + square
        depth = x.shape[1]
        deep = pl.ds(pl.multiple_of(source * depth, depth), depth)
        for e, rows_e in enumerate(by_expert(x * gain_ref[source])):
            rows_e = rows_e.astype(BF16)
            for n, w in enumerate((gate_w, up_w)):
                product = nn_dot(rows_e, w[e, deep, :])
                pre[h, e, n] = product if hop == 0 else pre[h, e, n] + product

    spread(0)
    for copy in loads[5:]:
        copy.wait()
    for h in range(2):
        expert_in(0, 0, h)

    y_1, y_2, y_3 = py >= 1, py >= 2, py >= 3
    x_1, x_2, x_3 = px >= 1, px >= 2, px >= 3

    def pieces(*cases):
        def work(m):
            taken = None
            for cond, places in cases:
                now = cond if taken is None else jnp.logical_and(cond, jnp.logical_not(taken))

                @pl.when(now)
                def _(places=places):
                    attend([held_at(a, b) for a, b in places], (m,))

                taken = cond if taken is None else jnp.logical_or(taken, cond)

        return [functools.partial(work, 0), functools.partial(work, 1)]

    both_2 = jnp.logical_and(x_2, y_2)
    mid = [
        *pieces((y_1, ((-1, -1), (-1, 1)))),
        *pieces((y_3, ((1, -1), (1, 1)))),
        *pieces((both_2, ((0, 2), (2, 0))), (x_2, ((0, 2),)), (y_2, ((2, 0),))),
    ]

    def rest():
        pass

    fillers = [
        *pieces((y_3, ((-1, 0), (1, 0))), (y_1, ((-1, 0),))),
        *pieces((x_3, ((0, -1), (0, 1))), (x_1, ((0, -1),))),
        lambda: spread(2),
        rest,
        *mid[:3],
        rest,
        *mid[3:],
        lambda: spread(3),
        *pieces((y_3, ((-1, 2), (1, 2))), (y_1, ((-1, 2),))),
        *pieces((y_2, ((2, -1), (2, 1)))),
    ]
    last_fillers = [lambda: spread(4), *pieces((y_2, ((2, 2),)))]

    def fill(count=1):
        for _ in range(count):
            if fillers:
                fillers.pop(0)()

    def activate(h):
        factor = lax.rsqrt(squares[h] / float(cfg["width"]) + NORM_EPS)
        for e, f in enumerate(by_expert(factor)):
            f = jnp.concatenate([f, f], axis=1)
            gate = jnp.minimum(pre[h, e, 0] * f, CLAMP_LIMIT)
            up = jnp.clip(pre[h, e, 1] * f, -CLAMP_LIMIT, CLAMP_LIMIT)
            hidden[2 * h + e] = ((up + 1.0) * gate * jax.nn.sigmoid(GLU_ALPHA * gate)).astype(
                BF16
            )

    for hop in range(1, far):
        for step in range(4):
            if (hop, step) == (2, 2):
                spread(1)
            for way in range(2):
                sub = sub_at(way, step)
                gather_wait(way, hop, sub)
                if sub in subs_of(way, hop):
                    gather_copy(way, hop, sub).start()
            if step % 2 == 1:
                for way in range(2):
                    partner_copy(way, hop, step // 2, c).start()
            if step == 0 and hop > 1:
                for way in range(2):
                    expert_in(way, hop - 1, 1)
            if step == 2:
                for way in range(2):
                    expert_in(way, hop, 0)
            if (hop, step) in ((2, 2), (2, 3), (3, 1), (3, 3)):
                fill()

    def gather_last(h):
        for way in range(2):
            gather_wait(way, far, 2 * h + way)
        partner_copy(0, far, h, c).start()

    goals = [ring(z, far)]
    for hop in range(1, far):
        goals += [ring(z, far - hop), ring(z, hop - far)]
    goals += [z]

    def goal_of(way, hop):
        return 0 if hop == 0 else 2 * hop - 1 + way

    def down(g, h):
        wide = pl.ds(pl.multiple_of(goals[g] * 256, 256), 256)
        for e in range(2):
            y = nn_dot(hidden[2 * h + e], down_w[e, :, wide]).astype(BF16)
            ybuf[0, g, 2 * h + e] = y[:, :128]
            ybuf[1, g, 2 * h + e] = y[:, 128:]
        y_copy(g, h).start()

    def y_copy(g, h):
        at = pl.ds(2 * h, 2)
        return remote(
            ybuf.at[1 - c, g, at],
            prec.at[g, at],
            y_send.at[0],
            y_recv.at[2 * g + h],
            ep,
            partner,
        )

    def sum_copy(way, hop, he):
        to = ring(z, 1) if way == 0 else ring(z, -1)
        at = (way * far + hop) * 4 + he
        return remote(
            rsend.at[at], rrecv.at[at], r_send.at[0], r_recv.at[at], ep, 2 * to + c
        )

    def own_sum(g, he):
        return ybuf[c, g, he].astype(F32) + prec[g, he].astype(F32)

    def arrived_sum(total, way, hop, he):
        if hop > 0 or he % 2 == way:
            sum_copy(way, hop, he).wait_recv()
            total = total + rrecv[(way * far + hop) * 4 + he].astype(F32)
        return total

    def pass_on(way, hop, he):
        total = own_sum(goal_of(way, hop), he)
        if hop > 0:
            total = arrived_sum(total, way, hop - 1, he)
        rsend[(way * far + hop) * 4 + he] = total.astype(BF16)
        sum_copy(way, hop, he).start()

    def begin(h):
        y_copy(0, h).wait_recv()
        for way in range(2):
            pass_on(way, 0, 2 * h + way)

    def fresh(h):
        for way in range(2):
            y_copy(goal_of(way, 1), h).wait_recv()
            pass_on(way, 1, 2 * h + 1 - way)

    def finish_expert(h):
        expert_in(0, far, h)
        activate(h)
        down(0, h)

    gather_last(0)
    for way in range(2):
        expert_in(way, far - 1, 1)
    finish_expert(0)
    for g in (1, 2):
        down(g, 0)
    gather_last(1)
    begin(0)
    finish_expert(1)
    fresh(0)
    for g in (1, 2):
        down(g, 1)
    begin(1)
    fresh(1)
    for g in (3, 4):
        for h in range(2):
            down(g, h)

    for hop in range(1, far):
        if hop > 1:
            for way in range(2):
                for h in range(2):
                    y_copy(goal_of(way, hop), h).wait_recv()
        for step in range(2 if hop == 1 else 0, 4):
            fill()
            for way in range(2):
                e = 1 - way if step < 2 else way
                pass_on(way, hop, step % 2 * 2 + e)
            if step == 2:
                for g in {1: (5, 6), 2: (7,), 3: ()}[hop]:
                    for h in range(2):
                        down(g, h)

    last = n_z - 1
    for h in range(2):
        y_copy(last, h).wait_recv()
    for h in range(2):
        totals = []
        for e in range(2):
            he = 2 * h + e
            if he == 0:
                fill(2)
            total = own_sum(last, he)
            for way in range(2):
                total = arrived_sum(total, way, far - 1, he)
            totals.append(total.reshape(sources_half, 1, cap, 128))
        back_send[h * half : (h + 1) * half] = (
            jnp.concatenate(totals, axis=1).reshape(half, 128).astype(BF16)
        )
        for p in reversed(range(h * sources_half, (h + 1) * sources_half)):

            @pl.when(px != p)
            def _(p=p):
                to = lax.rem(py + ROW_ORDER[p // SIDE] + SIDE, SIDE) * SIDE + p % SIDE
                remote(
                    back_send.at[pl.ds(p * block, block)],
                    back.at[mine],
                    b_sem.at[0],
                    b_sem.at[1],
                    to,
                    tp,
                ).start()

    back[mine, :] = back_send[own, :]
    fillers += last_fillers
    fill(len(fillers))

    mix = mix_ref[...]
    for r in range(0, q_rows, tile):
        one, two = pl.ds(r, tile), pl.ds(q_rows + r, tile)
        blend = acc[one, :width] / acc[one, width:] - mix * (acc[two, :width] / acc[two, width:])
        mean = jnp.mean(blend * blend, axis=1, keepdims=True)
        scaled = blend * lax.rsqrt(mean + SUB_EPS)
        attn_ref[one, :] = (scaled * sub_gain_ref[...] * OUT_SCALE).astype(BF16)

    sent = outgoing.at[pl.ds(0, others)]
    remote(sent, sent, d_send.at[0], d_recv.at[0], ep, partner).wait_send()
    for n, buf in enumerate((kbuf, vbuf)):
        whole = buf.at[pl.ds(0, n_ep - 1)]
        remote(whole, whole, kv_send.at[n], kv_recv.at[0], ep, partner).wait_send()
    whole = gathered.at[pl.ds(0, n_z - 1)]
    remote(whole, whole, g_send.at[0], g_recv.at[0], ep, partner).wait_send()
    whole = gathered.at[pl.ds(0, n_z)]
    remote(whole, whole, p_send.at[0], p_recv.at[0], ep, partner).wait_send()
    remote(ybuf.at[0], prec, y_send.at[0], y_recv.at[0], ep, partner).wait_send()
    sent = pl.ds(0, 4 * (n_z - 1))
    remote(rsend.at[sent], rrecv.at[sent], r_send.at[0], r_recv.at[0], ep, partner).wait_send()
    weight = jnp.concatenate(
        [pick_weight_ref[...], jnp.zeros((126, rows), F32)], axis=0
    ).T

    piece = back.at[pl.ds(0, others)]
    remote(piece, piece, b_sem.at[0], b_sem.at[1], ep, partner).wait()
    result = back[...]
    moe_ref[...] = (
        nn_dot(picks[0], result) * weight[:, 0:1] + nn_dot(picks[1], result) * weight[:, 1:2]
    ).astype(BF16)


def shards(
    queries,
    keys,
    values,
    mix_weight,
    sub_gain,
    tokens,
    routes,
    route_weights,
    expert_gain,
    gate_weight,
    up_weight,
    down_weight,
):
    n_ep, n_tp = lax.axis_size("ep"), lax.axis_size("tp")
    n_z = n_tp // 2
    rows, pick_count = routes.shape
    experts = n_ep * gate_weight.shape[0]
    cap = 3 * rows * pick_count // (2 * experts)
    slots = experts * cap
    part = slots // 4
    q_rows, _, qk_width = queries.shape
    v_width = values.shape[2]
    width = expert_gain.shape[0]
    ff = gate_weight.shape[2]
    cfg = dict(n_ep=n_ep, n_tp=n_tp, cap=cap, rows=rows, width=width)
    dma = pltpu.SemaphoreType.DMA
    vmem = pltpu.VMEM
    anywhere = pl.BlockSpec(memory_space=pl.ANY)
    whole = pl.BlockSpec(memory_space=vmem)
    attn_out, moe_out = pl.pallas_call(
        functools.partial(kernel, cfg),
        name="layer",
        out_shape=(
            vmem((q_rows, v_width), BF16),
            vmem((rows, tokens.shape[1]), BF16),
        ),
        in_specs=[anywhere] * 12,
        out_specs=(whole, whole),
        scratch_shapes=[
            vmem((q_rows, qk_width), BF16),
            vmem((1, 1), F32),
            vmem((1, v_width), F32),
            vmem(tokens.shape, BF16),
            vmem((pick_count, rows), jnp.int32),
            vmem((pick_count, rows), F32),
            vmem((n_z, 1, width // n_z), F32),
            vmem(gate_weight.shape, BF16),
            vmem(up_weight.shape, BF16),
            vmem(down_weight.shape, BF16),
            vmem((2 * q_rows, qk_width), BF16),
            vmem((n_ep, q_rows, qk_width), BF16),
            vmem((n_ep, q_rows, v_width), BF16),
            vmem((2 * q_rows, 2 * v_width), F32),
            vmem((2 * q_rows, 128), F32),
            vmem((2, rows, slots), BF16),
            vmem((slots, tokens.shape[1]), BF16),
            vmem((n_tp, slots, tokens.shape[1]), BF16),
            vmem((2, 2, 2, part, ff), F32),
            vmem((2, slots // 2, 128), F32),
            vmem((4, part, ff), BF16),
            vmem((2, n_z, 4, part, 128), BF16),
            vmem((n_z, 4, part, 128), BF16),
            vmem((4 * n_z, part, 128), BF16),
            vmem((4 * n_z, part, 128), BF16),
            vmem((slots, 128), BF16),
            vmem((slots, 128), BF16),
            dma((12,)),
            dma((2,)),
            dma((len(STAGES) - 1,)),
            dma((1,)),
            dma((SIDE,)),
            dma((1,)),
            dma((4 * n_z,)),
            dma((1,)),
            dma((2 * n_z,)),
            dma((1,)),
            dma((2 * n_z,)),
            dma((1,)),
            dma((4 * n_z,)),
            dma((2,)),
        ],
        compiler_params=pltpu.CompilerParams(
            collective_id=0, has_side_effects=True, vmem_limit_bytes=60 * 1024 * 1024
        ),
    )(
        queries.reshape(q_rows, qk_width),
        keys.reshape(q_rows, qk_width),
        values.reshape(q_rows, v_width),
        mix_weight.reshape(1, 1),
        sub_gain.reshape(1, v_width),
        tokens,
        routes.T,
        route_weights.T,
        expert_gain.reshape(n_z, 1, width // n_z),
        gate_weight,
        up_weight,
        down_weight,
    )
    return attn_out.reshape(q_rows, 1, v_width), moe_out


def solution(mesh):
    return jax.shard_map(
        shards,
        mesh=mesh,
        in_specs=(
            P("ep", "tp", None),
            P("ep", "tp", None),
            P("ep", "tp", None),
            P("tp"),
            P(),
            P("ep", "tp"),
            P("ep", None),
            P("ep", None),
            P(),
            P("ep", None, "tp"),
            P("ep", None, "tp"),
            P("ep", "tp", None),
        ),
        out_specs=(P("ep", "tp", None), P("ep", "tp")),
        check_vma=False,
    )
```
